256 devices in a mesh: fs: 32 (over z, x), rep: 4 (over y), tp: 2 (over core).
Axes of the slice: x: 4, y: 4, z: 8, core: 2. Of those that a mesh axis runs over, the one named last changes fastest.
Arguments:
- saved_input: bfloat16 [131072, 2048], P(('fs', 'rep')), may hold values from -24 to 24
- value_cotangent: bfloat16 [131072, 4096], P(('fs', 'rep'), 'tp'), may hold values from -0.0021972656 to 0.0021972656
- factor: bfloat16 [2048, 128], P('fs'), may hold values from -1.5 to 1.5
- weight: float32 [2048, 4096], P('fs', 'tp'), may hold values from -1.2 to 1.2
- first_moment: float32 [128, 4096], P('fs', 'tp'), may hold values from -1.8 to 1.8
- second_moment: float32 [128, 4096], P('fs', 'tp'), may hold values from 0.1 to 1
Outputs:
- low_grad: float32 [128, 4096], P('fs', 'tp')
- new_first: float32 [128, 4096], P('fs', 'tp')
- new_second: float32 [128, 4096], P('fs', 'tp')
- direction: float32 [2048, 4096], P('fs', 'tp')
- new_weight: float32 [2048, 4096], P('fs', 'tp')
- new_copy: bfloat16 [2048, 4096], P('fs', 'tp')
The draws below stay inside these ranges and needn't reach their ends.
All inputs are finite; a program needn't handle non-finite values.
Results may differ from the reference program's by a relative error of at most 0.006.
Values may be sent and summed in bfloat16 or wider, within the bound.
A program may use at most 64 MiB of HBM per device.

```python
import math
import jax
import jax.numpy as jnp
from jax import lax

D = 2048
E = 4096
R = 128
TOKENS = 131072


def with_spikes(entries, key, source, target, shards_of, factor):
    owner, partner = [(jnp.arange(entries.shape[axis_at]) // (entries.shape[axis_at] // shards_of)).reshape([-1 if axis == axis_at else 1 for axis in range(entries.ndim)]) for axis_at in (source, target)]
    chosen = jax.random.permutation(key, shards_of)[partner]
    strong = (owner == chosen) | (owner == (partner + shards_of // 2) % shards_of)
    return jnp.where(strong, factor * entries, entries)


def steps_of(own_key, shape, pieces, least, top_value):
    gain = 1.0
    for dim, shards_of in pieces:
        draws = jax.random.uniform(jax.random.fold_in(jax.random.fold_in(own_key, 6), dim), (shards_of,), jnp.float32, least / len(pieces), top_value / len(pieces))
        gain = gain * jnp.repeat(jnp.exp(draws), shape[dim] // shards_of).reshape((-1,) + (1,) * (len(shape) - 1 - dim))
    return gain


def gaussian(rng, shape, scale, most, cuts=(), kind=jnp.bfloat16):
    drawn = jax.random.normal(rng, shape, jnp.float32) * scale
    if len(cuts) > 0:
        drawn = steps_of(rng, shape, cuts, -0.22, 0.18) * drawn
    return jnp.clip(drawn, min=-most, max=most).astype(kind)


def heavy_noise(rng, extent, scale, limit, cuts, heavy, kind=jnp.bfloat16):
    entries = scale * jax.random.normal(rng, extent, jnp.float32)
    if cuts:
        entries = entries * steps_of(rng, extent, cuts, -0.22, 0.18)
    return jnp.clip(with_spikes(entries, jax.random.fold_in(rng, 3), *heavy), -limit, limit).astype(kind)


def setup_inputs(seed: int = 0) -> dict:
    key_of = jax.random.split(jax.random.key(seed), 7)
    saved_input = heavy_noise(key_of[0], (TOKENS, D), 1.0, 24.0, ((0, 128),), (0, 1, 128, 5.5))
    value_cotangent = gaussian(key_of[1], (TOKENS, E), (6.0 / (D * TOKENS) ** 0.5), 0.0021972656, ((0, 128), (1, 2)))
    factor = gaussian(key_of[2], (D, R), 0.25, 1.5, ((0, 32),))
    weight = gaussian(key_of[3], (D, E), 0.2, 1.2, ((0, 32), (1, 2)), jnp.float32)
    first_moment = gaussian(key_of[4], (R, E), 0.3, 1.8, ((0, 32), (1, 2)), jnp.float32)
    second_moment = jnp.clip(jnp.exp(math.log(1.0) - 2.3025851 * jax.random.uniform(key_of[5], (R, E), jnp.float32) ** steps_of(key_of[5], (R, E), ((0, 32), (1, 2)), -0.2, 0.2)), 0.1, 1.0)
    return dict(saved_input=saved_input, value_cotangent=value_cotangent, factor=factor, weight=weight, first_moment=first_moment, second_moment=second_moment)


first_decay = 0.9
second_decay = 0.9
learn_rate = 0.05
epsilon = 1e-08

def reference(saved_input, value_cotangent, factor, weight, first_moment, second_moment):
    grad = lax.dot_general(saved_input, value_cotangent, (((0,), (0,)), ((), ())), preferred_element_type=jnp.float32)
    factor_wide = factor.astype(jnp.float32)
    low_grad = lax.dot_general(factor_wide, grad, (((0,), (0,)), ((), ())), precision=lax.Precision.HIGHEST)
    new_first = first_decay * first_moment + (1.0 - first_decay) * low_grad
    new_second = second_decay * second_moment + (1.0 - second_decay) * low_grad * low_grad
    ratio = new_first / (jnp.sqrt(new_second) + epsilon)
    raw = jnp.dot(factor_wide, ratio, precision=lax.Precision.HIGHEST)
    spread = jnp.sqrt(jnp.sum(raw * raw) / (D * E))
    direction = raw / (spread + 1.0)
    new_weight = weight - learn_rate * direction
    return (low_grad, new_first, new_second, direction, new_weight, new_weight.astype(jnp.bfloat16))
```

```python
import functools

import jax
import jax.numpy as jnp
from jax import lax
from jax.experimental import pallas as pl
from jax.experimental.pallas import tpu as pltpu
from jax.sharding import PartitionSpec as P

MESH = pl.DeviceIdType.MESH
D = 2048
E = 4096
NX, NY, NZ = 4, 4, 8
PEERS = NX * NY
ROWS = 16
LANES = 128
OWNED = ROWS // NX
ZBLOCK = D // NZ
TOKENS = 1024
COLS = 2048
RANK = 128

first_decay = 0.9
second_decay = 0.9
learn_rate = 0.05
epsilon = 1e-08

PLANE = sorted(
    [(dx, dy) for dx in range(NX) for dy in range(NY) if (dx, dy) != (0, 0)],
    key=lambda d: -(min(d[0], NX - d[0]) + min(d[1], NY - d[1])),
)
Z_FAR = sorted(range(1, NZ), key=lambda d: -min(d, NZ - d))
Z_NEAR = [0] + Z_FAR[::-1]


def aligned(value, multiple):
    return pl.multiple_of(value * multiple, multiple)


def exchange_kernel(
    x_hbm, v_hbm, f_ref, fm_ref, sm_ref,
    rat_out, lg_out, tot_out,
    xv, vv, f_all, p_acc, pt, lsend, lrecv, zsend, zrecv, rat_all,
    mom_send, mom_recv, lg_send, lg_recv, tot_send, tot_recv,
    load_sem, out_sem, send_f, send_l, send_z, send_r, send_m, send_g, send_t,
    fz_sem, fxy_sem, lxy_sem, lz_sem, rz_sem, rxy_sem, m_sem, g_sem, t_sem,
):
    fs = lax.axis_index("fs")
    y = lax.axis_index("rep")
    tp = lax.axis_index("tp")
    x = lax.rem(fs, NX)
    z = lax.div(fs, NX)
    own = y * NX + x

    load_x = pltpu.make_async_copy(x_hbm, xv, load_sem.at[0])
    load_v = pltpu.make_async_copy(v_hbm, vv, load_sem.at[1])
    load_x.start()
    load_v.start()

    def plane_peer(dx, dy):
        px = lax.rem(x + dx, NX)
        py = lax.rem(y + dy, NY)
        return px, py, {"fs": z * NX + px, "rep": py}

    def z_peer(d):
        return {"fs": lax.rem(z + d, NZ) * NX + x}

    def send(src, dst, send_sem, recv_sem, device):
        pltpu.make_async_remote_copy(
            src_ref=src, dst_ref=dst, send_sem=send_sem, recv_sem=recv_sem,
            device_id=device, device_id_type=MESH,
        ).start()

    def drain(ref, sem):
        pltpu.make_async_copy(ref, ref, sem).wait()

    barrier = pltpu.get_barrier_semaphore()
    for d in Z_FAR:
        pl.semaphore_signal(barrier, inc=1, device_id=z_peer(d), device_id_type=MESH)
    for dx, dy in PLANE:
        pl.semaphore_signal(barrier, inc=1, device_id=plane_peer(dx, dy)[2], device_id_type=MESH)
    pl.semaphore_signal(barrier, inc=1, device_id={"tp": 1 - tp}, device_id_type=MESH)

    quarter = f_ref[pl.ds(aligned(y, ROWS), ROWS), :]
    f_own = pl.ds(aligned(z * PEERS + x * NY + y, ROWS), ROWS)
    f_all[f_own, :] = quarter
    for px in range(NX):
        cols = pl.ds(aligned(y * NX + px, LANES), LANES)
        mom_send[px, 0:OWNED, :] = fm_ref[:, cols]
        mom_send[px, OWNED:2 * OWNED, :] = sm_ref[:, cols]
    cols = pl.ds(aligned(own, LANES), LANES)
    mom_recv[x, 0:OWNED, :] = fm_ref[:, cols]
    mom_recv[x, OWNED:2 * OWNED, :] = sm_ref[:, cols]

    pl.semaphore_wait(barrier, NZ - 1 + PEERS - 1 + 1)

    for d in Z_FAR:
        send(f_all.at[f_own], f_all.at[f_own], send_f, fz_sem.at[NZ - d], z_peer(d))
    for d in Z_NEAR:
        zs = lax.rem(z + d, NZ)
        block = f_all.at[pl.ds(aligned(zs * PEERS + x * NY + y, ROWS), ROWS)]
        if d:
            drain(block, fz_sem.at[d])
        for dx, dy in PLANE:
            send(block, block, send_f, fxy_sem.at[d], plane_peer(dx, dy)[2])
    for dx in range(1, NX):
        px = lax.rem(x + dx, NX)
        send(mom_send.at[px], mom_recv.at[x], send_m, m_sem, {"fs": z * NX + px})

    load_x.wait()
    for step, d in enumerate(Z_NEAR):
        zs = lax.rem(z + d, NZ)
        rows = pl.ds(aligned(zs, ZBLOCK), ZBLOCK)
        drain(f_all.at[pl.ds(0, (PEERS - 1) * ROWS)], fxy_sem.at[d])
        term = jnp.dot(xv[:, rows], f_all[rows, :], preferred_element_type=jnp.float32)
        p_acc[...] = term if step == 0 else p_acc[...] + term
    projected = p_acc[...]
    upper = projected.astype(jnp.bfloat16)
    lower = (projected - upper.astype(jnp.float32)).astype(jnp.bfloat16)
    pt[0:RANK, :] = upper.T
    pt[RANK:, :] = lower.T

    load_v.wait()
    for dy in range(NY):
        py = lax.rem(y + NY - 1 - dy, NY)
        cols = pl.ds(aligned(py, NX * LANES), NX * LANES)
        both = jnp.dot(pt[...], vv[:, cols], preferred_element_type=jnp.float32)
        terms = (both[0:RANK] + both[RANK:]).astype(jnp.bfloat16)
        for zd in range(NZ):
            slot = lax.rem(zd - z + NZ, NZ)
            for px in range(NX):
                lsend[slot, py * NX + px] = terms[
                    zd * ROWS:(zd + 1) * ROWS, px * LANES:(px + 1) * LANES
                ]
    for d in Z_FAR + [0]:
        for dx, dy in PLANE:
            px, py, device = plane_peer(dx, dy)
            send(lsend.at[d, py * NX + px], lrecv.at[d, own], send_l, lxy_sem.at[d], device)

    whole = f_all[...]
    gram = lax.dot_general(whole, whole, (((0,), (0,)), ((), ())), preferred_element_type=jnp.float32)
    gram_1 = gram.astype(jnp.bfloat16)
    rest = gram - gram_1.astype(jnp.float32)
    gram_2 = rest.astype(jnp.bfloat16)
    gram_3 = (rest - gram_2.astype(jnp.float32)).astype(jnp.bfloat16)

    total = None
    for d in Z_FAR + [0]:
        drain(lrecv.at[d, pl.ds(0, PEERS - 1)], lxy_sem.at[d])
        lrecv[d, own] = lsend[d, own]
        summed = jnp.sum(lrecv[d].astype(jnp.float32), axis=0)
        if d:
            zsend[d] = summed.astype(jnp.bfloat16)
            send(zsend.at[d], zrecv.at[NZ - d], send_z, lz_sem.at[NZ - d], z_peer(d))
        else:
            total = summed
    for d in Z_NEAR[1:]:
        drain(zrecv.at[d], lz_sem.at[d])
        total = total + zrecv[d].astype(jnp.float32)

    drain(mom_recv.at[pl.ds(0, NX - 1)], m_sem)
    first = jnp.concatenate([mom_recv[i, 0:OWNED, :] for i in range(NX)], axis=0)
    second = jnp.concatenate([mom_recv[i, OWNED:2 * OWNED, :] for i in range(NX)], axis=0)
    new_first = first_decay * first + (1.0 - first_decay) * total
    new_second = second_decay * second + (1.0 - second_decay) * total * total
    ratio = new_first / (jnp.sqrt(new_second) + epsilon)
    tile_cols = pl.ds(aligned(own, LANES), LANES)
    rat_all[pl.ds(aligned(z, ROWS), ROWS), tile_cols] = ratio.astype(jnp.bfloat16)
    for i in range(NX):
        lg_send[i, 0:OWNED, :] = total[i * OWNED:(i + 1) * OWNED, :]
    lg_recv[own, 0:OWNED, :] = lg_send[x, 0:OWNED, :]

    tile = rat_all.at[pl.ds(aligned(z, ROWS), ROWS), tile_cols]
    for d in Z_FAR:
        send(tile, tile, send_r, rz_sem.at[NZ - d], z_peer(d))
    for d in Z_NEAR:
        zs = lax.rem(z + d, NZ)
        block = rat_all.at[pl.ds(aligned(zs, ROWS), ROWS), tile_cols]
        if d:
            drain(block, rz_sem.at[d])
        for dx, dy in PLANE:
            send(block, block, send_r, rxy_sem.at[d], plane_peer(dx, dy)[2])
    for dx, dy in PLANE:
        px, py, device = plane_peer(dx, dy)
        send(lg_send.at[px], lg_recv.at[own], send_g, g_sem, device)
    for d in Z_NEAR:
        drain(lrecv.at[d, pl.ds(0, PEERS - 1)], rxy_sem.at[d])

    ratio_whole = rat_all[...]
    squares = jnp.zeros((8, LANES), jnp.float32)
    for c in range(COLS // 512):
        part = ratio_whole[:, c * 512:(c + 1) * 512]
        mixed = (
            jnp.dot(gram_1, part, preferred_element_type=jnp.float32)
            + jnp.dot(gram_2, part, preferred_element_type=jnp.float32)
            + jnp.dot(gram_3, part, preferred_element_type=jnp.float32)
        ) * part.astype(jnp.float32)
        for k in range(4):
            squares = squares + jnp.sum(
                mixed[:, k * LANES:(k + 1) * LANES].reshape(RANK // 8, 8, LANES), axis=0
            )
    tot_send[...] = squares
    send(tot_send, tot_recv, send_t, t_sem, {"tp": 1 - tp})
    save = pltpu.make_async_copy(rat_all, rat_out, out_sem)
    save.start()
    drain(lg_recv.at[pl.ds(0, PEERS - 1)], g_sem)
    lg_out[...] = lg_recv[...]
    drain(tot_recv, t_sem)
    tot_out[...] = squares + tot_recv[...]

    save.wait()
    drain(f_all.at[pl.ds(0, (NZ - 1) * ROWS)], send_f)
    for d in range(NZ):
        drain(f_all.at[pl.ds(0, (PEERS - 1) * ROWS)], send_f)
    drain(lsend.at[:, pl.ds(0, PEERS - 1)], send_l)
    drain(zsend.at[pl.ds(0, NZ - 1)], send_z)
    drain(zsend.at[pl.ds(0, NZ - 1)], send_r)
    drain(lsend.at[:, pl.ds(0, PEERS - 1)], send_r)
    drain(mom_send.at[pl.ds(0, NX - 1)], send_m)
    drain(lg_recv.at[pl.ds(0, PEERS - 1)], send_g)
    drain(tot_send, send_t)


def exchange(saved_input, value_cotangent, factor, first_moment, second_moment):
    bf16, f32 = jnp.bfloat16, jnp.float32
    dma = pltpu.SemaphoreType.DMA
    vmem = pl.BlockSpec(memory_space=pltpu.VMEM)
    hbm = pl.BlockSpec(memory_space=pl.ANY)
    return pl.pallas_call(
        exchange_kernel,
        out_shape=(
            jax.ShapeDtypeStruct((RANK, COLS), bf16),
            jax.ShapeDtypeStruct((PEERS, 8, LANES), f32),
            jax.ShapeDtypeStruct((8, LANES), f32),
        ),
        in_specs=[hbm, hbm, vmem, vmem, vmem],
        out_specs=(hbm, vmem, vmem),
        scratch_shapes=[
            pltpu.VMEM((TOKENS, D), bf16),
            pltpu.VMEM((TOKENS, COLS), bf16),
            pltpu.VMEM((D, RANK), bf16),
            pltpu.VMEM((TOKENS, RANK), f32),
            pltpu.VMEM((2 * RANK, TOKENS), bf16),
            pltpu.VMEM((NZ, PEERS, ROWS, LANES), bf16),
            pltpu.VMEM((NZ, PEERS, ROWS, LANES), bf16),
            pltpu.VMEM((NZ, ROWS, LANES), bf16),
            pltpu.VMEM((NZ, ROWS, LANES), bf16),
            pltpu.VMEM((RANK, COLS), bf16),
            pltpu.VMEM((NX, 8, LANES), f32),
            pltpu.VMEM((NX, 8, LANES), f32),
            pltpu.VMEM((NX, 8, LANES), f32),
            pltpu.VMEM((PEERS, 8, LANES), f32),
            pltpu.VMEM((8, LANES), f32),
            pltpu.VMEM((8, LANES), f32),
            dma((2,)),
        ] + [dma] * 8 + [dma((NZ,))] * 6 + [dma] * 3,
        compiler_params=pltpu.CompilerParams(
            collective_id=0, has_side_effects=True, vmem_limit_bytes=40 * 2**20
        ),
    )(saved_input, value_cotangent, factor, first_moment, second_moment)


def update_kernel(
    f_ref, rat_ref, lg_ref, tot_ref, w_ref, fm_ref, sm_ref,
    low_ref, first_ref, second_ref, dir_ref, weight_ref, copy_ref,
):
    total = jnp.sum(tot_ref[...], axis=(0, 1), keepdims=True)
    spread = jnp.sqrt(total / (D * E))
    raw = jnp.dot(f_ref[...], rat_ref[...], preferred_element_type=jnp.float32)
    direction = raw / (spread + 1.0)
    new_weight = w_ref[...] - learn_rate * direction
    dir_ref[...] = direction
    weight_ref[...] = new_weight
    copy_ref[...] = new_weight.astype(jnp.bfloat16)
    for j in range(PEERS):
        cols = slice(j * LANES, (j + 1) * LANES)
        low = lg_ref[j, 0:OWNED, :]
        low_ref[:, cols] = low
        first_ref[:, cols] = first_decay * fm_ref[:, cols] + (1.0 - first_decay) * low
        second_ref[:, cols] = second_decay * sm_ref[:, cols] + (1.0 - second_decay) * low * low


def update(factor, ratio, low, total, weight, first_moment, second_moment):
    f32 = jnp.float32
    rows = factor.shape[0]
    vmem = pl.BlockSpec(memory_space=pltpu.VMEM)
    small = jax.ShapeDtypeStruct((OWNED, COLS), f32)
    large = jax.ShapeDtypeStruct((rows, COLS), f32)
    return pl.pallas_call(
        update_kernel,
        out_shape=(small, small, small, large, large, jax.ShapeDtypeStruct((rows, COLS), jnp.bfloat16)),
        in_specs=[vmem] * 7,
        out_specs=(vmem,) * 6,
    )(factor, ratio, low, total, weight, first_moment, second_moment)


def on_device(saved_input, value_cotangent, factor, weight, first_moment, second_moment):
    ratio, low, total = exchange(saved_input, value_cotangent, factor, first_moment, second_moment)
    return update(factor, ratio, low, total, weight, first_moment, second_moment)


def solution(mesh):
    placed = (
        P(("fs", "rep"), None),
        P(("fs", "rep"), "tp"),
        P("fs", None),
        P("fs", "tp"),
        P("fs", "tp"),
        P("fs", "tp"),
    )
    return jax.shard_map(
        on_device,
        mesh=mesh,
        in_specs=placed,
        out_specs=(P("fs", "tp"),) * 6,
        check_vma=False,
    )
```

```python
import functools

import jax
import jax.numpy as jnp
from jax import lax
from jax.experimental import pallas as pl
from jax.experimental.pallas import tpu as pltpu
from jax.sharding import PartitionSpec as P

MESH = pl.DeviceIdType.MESH
D = 2048
E = 4096
NX, NY, NZ = 4, 4, 8
PEERS = NX * NY
ROWS = 16
LANES = 128
OWNED = ROWS // NX
ZBLOCK = D // NZ
TOKENS = 1024
COLS = 2048
RANK = 128

first_decay = 0.9
second_decay = 0.9
learn_rate = 0.05
epsilon = 1e-08

PLANE = sorted(
    [(dx, dy) for dx in range(NX) for dy in range(NY) if (dx, dy) != (0, 0)],
    key=lambda d: -(min(d[0], NX - d[0]) + min(d[1], NY - d[1])),
)
Z_FAR = sorted(range(1, NZ), key=lambda d: -min(d, NZ - d))
Z_NEAR = [0] + Z_FAR[::-1]


def aligned(value, multiple):
    return pl.multiple_of(value * multiple, multiple)


def exchange_kernel(
    x_hbm, v_hbm, f_hbm, fm_hbm, sm_hbm,
    rat_out, lg_out, tot_out,
    f_ref, fm_ref, sm_ref, xv, vv, f_all, p_acc, pt, lsend, lrecv, zsend, zrecv, rat_all,
    mom_send, mom_recv, lg_send, lg_recv, tot_send, tot_recv,
    load_sem, send_f, send_l, send_z, send_r, send_m, send_g, send_t,
    fz_sem, fxy_sem, lxy_sem, lz_sem, rz_sem, rxy_sem, m_sem, g_sem, t_sem,
):
    fs = lax.axis_index("fs")
    y = lax.axis_index("rep")
    tp = lax.axis_index("tp")
    x = lax.rem(fs, NX)
    z = lax.div(fs, NX)
    own = y * NX + x

    load_f = pltpu.make_async_copy(f_hbm, f_ref, load_sem.at[2])
    load_fm = pltpu.make_async_copy(fm_hbm, fm_ref, load_sem.at[3])
    load_sm = pltpu.make_async_copy(sm_hbm, sm_ref, load_sem.at[4])
    load_x = pltpu.make_async_copy(x_hbm, xv, load_sem.at[0])
    load_v = pltpu.make_async_copy(v_hbm, vv, load_sem.at[1])
    for load in (load_f, load_fm, load_sm, load_x, load_v):
        load.start()

    def plane_peer(dx, dy):
        px = lax.rem(x + dx, NX)
        py = lax.rem(y + dy, NY)
        return px, py, {"fs": z * NX + px, "rep": py}

    def z_peer(d):
        return {"fs": lax.rem(z + d, NZ) * NX + x}

    def send(src, dst, send_sem, recv_sem, device):
        pltpu.make_async_remote_copy(
            src_ref=src, dst_ref=dst, send_sem=send_sem, recv_sem=recv_sem,
            device_id=device, device_id_type=MESH,
        ).start()

    def drain(ref, sem):
        pltpu.make_async_copy(ref, ref, sem).wait()

    barrier = pltpu.get_barrier_semaphore()
    for d in Z_FAR:
        pl.semaphore_signal(barrier, inc=1, device_id=z_peer(d), device_id_type=MESH)
    for dx, dy in PLANE:
        pl.semaphore_signal(barrier, inc=1, device_id=plane_peer(dx, dy)[2], device_id_type=MESH)
    pl.semaphore_signal(barrier, inc=1, device_id={"tp": 1 - tp}, device_id_type=MESH)

    load_f.wait()
    load_fm.wait()
    load_sm.wait()
    quarter = f_ref[pl.ds(aligned(y, ROWS), ROWS), :]
    f_own = pl.ds(aligned(z * PEERS + x * NY + y, ROWS), ROWS)
    f_all[f_own, :] = quarter
    for px in range(NX):
        cols = pl.ds(aligned(y * NX + px, LANES), LANES)
        mom_send[px, 0:OWNED, :] = fm_ref[:, cols]
        mom_send[px, OWNED:2 * OWNED, :] = sm_ref[:, cols]
    cols = pl.ds(aligned(own, LANES), LANES)
    mom_recv[x, 0:OWNED, :] = fm_ref[:, cols]
    mom_recv[x, OWNED:2 * OWNED, :] = sm_ref[:, cols]

    pl.semaphore_wait(barrier, NZ - 1 + PEERS - 1 + 1)

    for d in Z_FAR:
        send(f_all.at[f_own], f_all.at[f_own], send_f, fz_sem.at[NZ - d], z_peer(d))
    for d in Z_NEAR:
        zs = lax.rem(z + d, NZ)
        block = f_all.at[pl.ds(aligned(zs * PEERS + x * NY + y, ROWS), ROWS)]
        if d:
            drain(block, fz_sem.at[d])
        for dx, dy in PLANE:
            send(block, block, send_f, fxy_sem.at[d], plane_peer(dx, dy)[2])
    for dx in range(1, NX):
        px = lax.rem(x + dx, NX)
        send(mom_send.at[px], mom_recv.at[x], send_m, m_sem, {"fs": z * NX + px})

    load_x.wait()
    for step, d in enumerate(Z_NEAR):
        zs = lax.rem(z + d, NZ)
        rows = pl.ds(aligned(zs, ZBLOCK), ZBLOCK)
        drain(f_all.at[pl.ds(0, (PEERS - 1) * ROWS)], fxy_sem.at[d])
        term = jnp.dot(xv[:, rows], f_all[rows, :], preferred_element_type=jnp.float32)
        p_acc[...] = term if step == 0 else p_acc[...] + term
    projected = p_acc[...]
    upper = projected.astype(jnp.bfloat16)
    lower = (projected - upper.astype(jnp.float32)).astype(jnp.bfloat16)
    pt[0:RANK, :] = upper.T
    pt[RANK:, :] = lower.T

    load_v.wait()
    for dy in range(NY):
        py = lax.rem(y + NY - 1 - dy, NY)
        cols = pl.ds(aligned(py, NX * LANES), NX * LANES)
        both = jnp.dot(pt[...], vv[:, cols], preferred_element_type=jnp.float32)
        terms = (both[0:RANK] + both[RANK:]).astype(jnp.bfloat16)
        for zd in range(NZ):
            slot = lax.rem(zd - z + NZ, NZ)
            for px in range(NX):
                lsend[slot, py * NX + px] = terms[
                    zd * ROWS:(zd + 1) * ROWS, px * LANES:(px + 1) * LANES
                ]
    for d in Z_FAR + [0]:
        for dx, dy in PLANE:
            px, py, device = plane_peer(dx, dy)
            send(lsend.at[d, py * NX + px], lrecv.at[d, own], send_l, lxy_sem.at[d], device)

    whole = f_all[...]
    gram = lax.dot_general(whole, whole, (((0,), (0,)), ((), ())), preferred_element_type=jnp.float32)
    gram_1 = gram.astype(jnp.bfloat16)
    rest = gram - gram_1.astype(jnp.float32)
    gram_2 = rest.astype(jnp.bfloat16)
    gram_3 = (rest - gram_2.astype(jnp.float32)).astype(jnp.bfloat16)

    total = None
    for d in Z_FAR + [0]:
        drain(lrecv.at[d, pl.ds(0, PEERS - 1)], lxy_sem.at[d])
        lrecv[d, own] = lsend[d, own]
        summed = jnp.sum(lrecv[d].astype(jnp.float32), axis=0)
        if d:
            zsend[d] = summed.astype(jnp.bfloat16)
            send(zsend.at[d], zrecv.at[NZ - d], send_z, lz_sem.at[NZ - d], z_peer(d))
        else:
            total = summed
    for d in Z_NEAR[1:]:
        drain(zrecv.at[d], lz_sem.at[d])
        total = total + zrecv[d].astype(jnp.float32)

    drain(mom_recv.at[pl.ds(0, NX - 1)], m_sem)
    first = jnp.concatenate([mom_recv[i, 0:OWNED, :] for i in range(NX)], axis=0)
    second = jnp.concatenate([mom_recv[i, OWNED:2 * OWNED, :] for i in range(NX)], axis=0)
    new_first = first_decay * first + (1.0 - first_decay) * total
    new_second = second_decay * second + (1.0 - second_decay) * total * total
    ratio = new_first / (jnp.sqrt(new_second) + epsilon)
    tile_cols = pl.ds(aligned(own, LANES), LANES)
    rat_all[pl.ds(aligned(z, ROWS), ROWS), tile_cols] = ratio.astype(jnp.bfloat16)
    for i in range(NX):
        lg_send[i, 0:OWNED, :] = total[i * OWNED:(i + 1) * OWNED, :]
    lg_recv[own, 0:OWNED, :] = lg_send[x, 0:OWNED, :]

    tile = rat_all.at[pl.ds(aligned(z, ROWS), ROWS), tile_cols]
    for d in Z_FAR:
        send(tile, tile, send_r, rz_sem.at[NZ - d], z_peer(d))
    for d in Z_NEAR:
        zs = lax.rem(z + d, NZ)
        block = rat_all.at[pl.ds(aligned(zs, ROWS), ROWS), tile_cols]
        if d:
            drain(block, rz_sem.at[d])
        for dx, dy in PLANE:
            send(block, block, send_r, rxy_sem.at[d], plane_peer(dx, dy)[2])
    for dx, dy in PLANE:
        px, py, device = plane_peer(dx, dy)
        send(lg_send.at[px], lg_recv.at[own], send_g, g_sem, device)
    for d in Z_NEAR:
        drain(lrecv.at[d, pl.ds(0, PEERS - 1)], rxy_sem.at[d])

    ratio_whole = rat_all[...]
    squares = jnp.zeros((8, LANES), jnp.float32)
    for c in range(COLS // 512):
        part = ratio_whole[:, c * 512:(c + 1) * 512]
        mixed = (
            jnp.dot(gram_1, part, preferred_element_type=jnp.float32)
            + jnp.dot(gram_2, part, preferred_element_type=jnp.float32)
            + jnp.dot(gram_3, part, preferred_element_type=jnp.float32)
        ) * part.astype(jnp.float32)
        for k in range(4):
            squares = squares + jnp.sum(
                mixed[:, k * LANES:(k + 1) * LANES].reshape(RANK // 8, 8, LANES), axis=0
            )
    tot_send[...] = squares
    send(tot_send, tot_recv, send_t, t_sem, {"tp": 1 - tp})
    rat_out[...] = ratio_whole
    drain(lg_recv.at[pl.ds(0, PEERS - 1)], g_sem)
    lg_out[...] = lg_recv[...]
    drain(tot_recv, t_sem)
    tot_out[...] = squares + tot_recv[...]

    drain(f_all.at[pl.ds(0, (NZ - 1) * ROWS)], send_f)
    for d in range(NZ):
        drain(f_all.at[pl.ds(0, (PEERS - 1) * ROWS)], send_f)
    drain(lsend.at[:, pl.ds(0, PEERS - 1)], send_l)
    drain(zsend.at[pl.ds(0, NZ - 1)], send_z)
    drain(zsend.at[pl.ds(0, NZ - 1)], send_r)
    drain(lsend.at[:, pl.ds(0, PEERS - 1)], send_r)
    drain(mom_send.at[pl.ds(0, NX - 1)], send_m)
    drain(lg_recv.at[pl.ds(0, PEERS - 1)], send_g)
    drain(tot_send, send_t)


def exchange(saved_input, value_cotangent, factor, first_moment, second_moment):
    bf16, f32 = jnp.bfloat16, jnp.float32
    dma = pltpu.SemaphoreType.DMA
    vmem = pl.BlockSpec(memory_space=pltpu.VMEM)
    hbm = pl.BlockSpec(memory_space=pltpu.HBM)
    return pl.pallas_call(
        exchange_kernel,
        out_shape=(
            jax.ShapeDtypeStruct((RANK, COLS), bf16),
            jax.ShapeDtypeStruct((PEERS, 8, LANES), f32),
            jax.ShapeDtypeStruct((8, LANES), f32),
        ),
        in_specs=[hbm] * 5,
        out_specs=(vmem,) * 3,
        scratch_shapes=[
            pltpu.VMEM((D // (NX * NZ), RANK), bf16),
            pltpu.VMEM((OWNED, COLS), f32),
            pltpu.VMEM((OWNED, COLS), f32),
            pltpu.VMEM((TOKENS, D), bf16),
            pltpu.VMEM((TOKENS, COLS), bf16),
            pltpu.VMEM((D, RANK), bf16),
            pltpu.VMEM((TOKENS, RANK), f32),
            pltpu.VMEM((2 * RANK, TOKENS), bf16),
            pltpu.VMEM((NZ, PEERS, ROWS, LANES), bf16),
            pltpu.VMEM((NZ, PEERS, ROWS, LANES), bf16),
            pltpu.VMEM((NZ, ROWS, LANES), bf16),
            pltpu.VMEM((NZ, ROWS, LANES), bf16),
            pltpu.VMEM((RANK, COLS), bf16),
            pltpu.VMEM((NX, 8, LANES), f32),
            pltpu.VMEM((NX, 8, LANES), f32),
            pltpu.VMEM((NX, 8, LANES), f32),
            pltpu.VMEM((PEERS, 8, LANES), f32),
            pltpu.VMEM((8, LANES), f32),
            pltpu.VMEM((8, LANES), f32),
            dma((5,)),
        ] + [dma] * 7 + [dma((NZ,))] * 6 + [dma] * 3,
        compiler_params=pltpu.CompilerParams(
            collective_id=0, has_side_effects=True, vmem_limit_bytes=32 * 2**20
        ),
    )(*(
        pltpu.with_memory_space_constraint(a, pltpu.HBM)
        for a in (saved_input, value_cotangent, factor, first_moment, second_moment)
    ))


def update_kernel(
    f_ref, rat_ref, lg_ref, tot_ref, w_ref, fm_ref, sm_ref,
    low_ref, first_ref, second_ref, dir_ref, weight_ref, copy_ref,
):
    total = jnp.sum(tot_ref[...], axis=(0, 1), keepdims=True)
    spread = jnp.sqrt(total / (D * E))
    raw = jnp.dot(f_ref[...], rat_ref[...], preferred_element_type=jnp.float32)
    direction = raw / (spread + 1.0)
    new_weight = w_ref[...] - learn_rate * direction
    dir_ref[...] = direction
    weight_ref[...] = new_weight
    copy_ref[...] = new_weight.astype(jnp.bfloat16)
    for j in range(PEERS):
        cols = slice(j * LANES, (j + 1) * LANES)
        low = lg_ref[j, 0:OWNED, :]
        low_ref[:, cols] = low
        first_ref[:, cols] = first_decay * fm_ref[:, cols] + (1.0 - first_decay) * low
        second_ref[:, cols] = second_decay * sm_ref[:, cols] + (1.0 - second_decay) * low * low


def update(factor, ratio, low, total, weight, first_moment, second_moment):
    f32 = jnp.float32
    rows = factor.shape[0]
    vmem = pl.BlockSpec(memory_space=pltpu.VMEM)
    small = jax.ShapeDtypeStruct((OWNED, COLS), f32)
    large = jax.ShapeDtypeStruct((rows, COLS), f32)
    return pl.pallas_call(
        update_kernel,
        out_shape=(small, small, small, large, large, jax.ShapeDtypeStruct((rows, COLS), jnp.bfloat16)),
        in_specs=[vmem] * 7,
        out_specs=(vmem,) * 6,
        compiler_params=pltpu.CompilerParams(vmem_limit_bytes=8 * 2**20),
    )(factor, ratio, low, total, weight, first_moment, second_moment)


def on_device(saved_input, value_cotangent, factor, weight, first_moment, second_moment):
    ratio, low, total = exchange(saved_input, value_cotangent, factor, first_moment, second_moment)
    return update(factor, ratio, low, total, weight, first_moment, second_moment)


def solution(mesh):
    placed = (
        P(("fs", "rep"), None),
        P(("fs", "rep"), "tp"),
        P("fs", None),
        P("fs", "tp"),
        P("fs", "tp"),
        P("fs", "tp"),
    )
    return jax.shard_map(
        on_device,
        mesh=mesh,
        in_specs=placed,
        out_specs=(P("fs", "tp"),) * 6,
        check_vma=False,
    )
```

```python
import functools

import jax
import jax.numpy as jnp
from jax import lax
from jax.experimental import pallas as pl
from jax.experimental.pallas import tpu as pltpu
from jax.sharding import PartitionSpec as P

MESH = pl.DeviceIdType.MESH
D = 2048
E = 4096
NX, NY, NZ = 4, 4, 8
PEERS = NX * NY
ROWS = 16
LANES = 128
OWNED = ROWS // NX
ZBLOCK = D // NZ
TOKENS = 1024
COLS = 2048
RANK = 128

first_decay = 0.9
second_decay = 0.9
learn_rate = 0.05
epsilon = 1e-08

PLANE = sorted(
    [(dx, dy) for dx in range(NX) for dy in range(NY) if (dx, dy) != (0, 0)],
    key=lambda d: -(min(d[0], NX - d[0]) + min(d[1], NY - d[1])),
)
Z_FAR = [4, 3, 5, 2, 6, 1, 7]
GROUPS = [(0,), (1, 7), (2, 6), (3, 5), (4,)]
BASE = [PEERS * sum(len(g) for g in GROUPS[:i]) for i in range(len(GROUPS))]
GROUP_OF = {d: (i, k) for i, g in enumerate(GROUPS) for k, d in enumerate(g)}
PARTS = [(4, 3, 5), (2, 6, 1, 7, 0)]
ORDER = [d for part in PARTS for d in part]
NEAR = [0, 3, 1, 2]


def aligned(value, multiple):
    return pl.multiple_of(value * multiple, multiple)


def exchange_kernel(
    x_hbm, v_hbm, f_hbm, fm_hbm, sm_hbm,
    rat_out, lg_out, tot_out,
    f_ref, fm_ref, sm_ref, xv, vv, fbuf, p_acc, pt, lsend, lrecv, zsend, zrecv, rbuf, column,
    mom_send, mom_recv, lg_send, lg_recv, square, squares,
    load_sem, send_f, send_l, send_z, send_r, send_m, send_g, send_q,
    fz_sem, fxy_sem, lxy_sem, lz_sem, rz_sem, rxy_sem, m_sem, g_sem, q_sem,
):
    fs = lax.axis_index("fs")
    y = lax.axis_index("rep")
    tp = lax.axis_index("tp")
    x = lax.rem(fs, NX)
    z = lax.div(fs, NX)
    own = y * NX + x
    own_f = x * NY + y

    def plane_peer(dx, dy):
        px = lax.rem(x + dx, NX)
        py = lax.rem(y + dy, NY)
        return px, py, {"fs": z * NX + px, "rep": py}

    def z_peer(d):
        return {"fs": lax.rem(z + d, NZ) * NX + x}

    def send(src, dst, send_sem, recv_sem, device):
        pltpu.make_async_remote_copy(
            src_ref=src, dst_ref=dst, send_sem=send_sem, recv_sem=recv_sem,
            device_id=device, device_id_type=MESH,
        ).start()

    def drain(ref, sem):
        pltpu.make_async_copy(ref, ref, sem).wait()

    barrier = pltpu.get_barrier_semaphore()
    for d in Z_FAR:
        pl.semaphore_signal(barrier, inc=1, device_id=z_peer(d), device_id_type=MESH)
    for dx, dy in PLANE:
        device = plane_peer(dx, dy)[2]
        pl.semaphore_signal(barrier, inc=1, device_id=device, device_id_type=MESH)
        pl.semaphore_signal(barrier, inc=1, device_id={**device, "tp": 1 - tp}, device_id_type=MESH)
    pl.semaphore_signal(barrier, inc=1, device_id={"tp": 1 - tp}, device_id_type=MESH)

    load_f = pltpu.make_async_copy(f_hbm, f_ref, load_sem.at[2])
    load_fm = pltpu.make_async_copy(fm_hbm, fm_ref, load_sem.at[3])
    load_sm = pltpu.make_async_copy(sm_hbm, sm_ref, load_sem.at[4])
    load_x = pltpu.make_async_copy(x_hbm, xv, load_sem.at[0])
    load_v = pltpu.make_async_copy(v_hbm, vv, load_sem.at[1])
    for load in (load_f, load_fm, load_sm, load_x, load_v):
        load.start()

    load_f.wait()
    fbuf[own_f] = f_ref[pl.ds(aligned(y, ROWS), ROWS), :]
    load_fm.wait()
    load_sm.wait()
    for px in range(NX):
        cols = pl.ds(aligned(y * NX + px, LANES), LANES)
        mom_send[px, 0:OWNED, :] = fm_ref[:, cols]
        mom_send[px, OWNED:2 * OWNED, :] = sm_ref[:, cols]
    cols = pl.ds(aligned(own, LANES), LANES)
    mom_recv[x, 0:OWNED, :] = fm_ref[:, cols]
    mom_recv[x, OWNED:2 * OWNED, :] = sm_ref[:, cols]

    pl.semaphore_wait(barrier, NZ - 1 + 2 * (PEERS - 1) + 1)

    def gather_z(buf, slot, send_sem, z_sem):
        for d in Z_FAR:
            i, k = GROUP_OF[NZ - d]
            dst = buf.at[BASE[i] + slot * len(GROUPS[i]) + k]
            send(buf.at[slot], dst, send_sem, z_sem.at[NZ - d], z_peer(d))

    def gather_plane(buf, slot, i, send_sem, z_sem, plane_sem):
        n = len(GROUPS[i])
        block = buf.at[pl.ds(BASE[i] + slot * n, n)]
        for d in GROUPS[i]:
            if d:
                drain(buf.at[0], z_sem.at[d])
        for dx, dy in PLANE:
            send(block, block, send_sem, plane_sem.at[i], plane_peer(dx, dy)[2])

    def arrived(buf, i, plane_sem):
        n = len(GROUPS[i])
        drain(buf.at[pl.ds(0, (PEERS - 1) * n)], plane_sem.at[i])
        return buf[BASE[i]:BASE[i] + PEERS * n].reshape(PEERS, n, ROWS, LANES)

    gather_z(fbuf, own_f, send_f, fz_sem)
    for i in range(len(GROUPS)):
        gather_plane(fbuf, own_f, i, send_f, fz_sem, fxy_sem)
    for dx in range(1, NX):
        px = lax.rem(x + dx, NX)
        send(mom_send.at[px], mom_recv.at[x], send_m, m_sem, {"fs": z * NX + px})

    load_x.wait()
    for i, group in enumerate(GROUPS):
        blocks = arrived(fbuf, i, fxy_sem)
        term = p_acc[...] if i else None
        for k, d in enumerate(group):
            columns = xv[:, pl.ds(aligned(lax.rem(z + d, NZ), ZBLOCK), ZBLOCK)]
            block = blocks[:, k].reshape(ZBLOCK, RANK)
            product = jnp.dot(columns, block, preferred_element_type=jnp.float32)
            term = product if term is None else term + product
        p_acc[...] = term
    projected = p_acc[...]
    upper = projected.astype(jnp.bfloat16)
    lower = (projected - upper.astype(jnp.float32)).astype(jnp.bfloat16)
    pt[0:RANK, :] = upper.T
    pt[RANK:, :] = lower.T

    def send_part(part, dy):
        begin = sum(len(p) for p in PARTS[:part])
        for dx in NEAR[::-1]:
            if dx or dy:
                px, py, device = plane_peer(dx, dy)
                src = lsend.at[py * NX + px, pl.ds(begin, len(PARTS[part]))]
                dst = lrecv.at[own, pl.ds(begin, len(PARTS[part]))]
                send(src, dst, send_l, lxy_sem.at[part], device)

    load_v.wait()
    chunks = [2, 1, 3, 0]
    for step, dy in enumerate(chunks):
        py = lax.rem(y + dy, NY)
        cols = pl.ds(aligned(py, NX * LANES), NX * LANES)
        both = jnp.dot(pt[...], vv[:, cols], preferred_element_type=jnp.float32)
        pt_terms = (both[0:RANK] + both[RANK:]).astype(jnp.bfloat16)
        terms = pt_terms.reshape(NZ, ROWS, NX * LANES)
        column[...] = terms
        for slot, d in enumerate(ORDER):
            rows = column[lax.rem(z + d, NZ)]
            for px in range(NX):
                lsend[py * NX + px, slot] = rows[:, px * LANES:(px + 1) * LANES]
        send_part(0, dy)
        if step == 2:
            send_part(1, chunks[0])
    for dy in chunks[1:]:
        send_part(1, dy)
    lrecv[own] = lsend[own]

    whole = fbuf[...].reshape(D, RANK)
    gram = lax.dot_general(whole, whole, (((0,), (0,)), ((), ())), preferred_element_type=jnp.float32)
    gram_1 = gram.astype(jnp.bfloat16)
    rest = gram - gram_1.astype(jnp.float32)
    gram_2 = rest.astype(jnp.bfloat16)
    gram_3 = (rest - gram_2.astype(jnp.float32)).astype(jnp.bfloat16)

    total = None
    for slot, d in enumerate(ORDER):
        for part, group in enumerate(PARTS):
            if d == group[0]:
                drain(lrecv.at[pl.ds(0, PEERS - 1), pl.ds(0, len(group))], lxy_sem.at[part])
        summed = jnp.sum(lrecv[:, slot].astype(jnp.float32), axis=0)
        if d:
            zsend[d] = summed.astype(jnp.bfloat16)
            send(zsend.at[d], zrecv.at[NZ - d], send_z, lz_sem.at[NZ - d], z_peer(d))
        else:
            total = summed
    drain(mom_recv.at[pl.ds(0, NX - 1)], m_sem)
    first = jnp.concatenate([mom_recv[i, 0:OWNED, :] for i in range(NX)], axis=0)
    second = jnp.concatenate([mom_recv[i, OWNED:2 * OWNED, :] for i in range(NX)], axis=0)
    for d in Z_FAR[::-1]:
        drain(zrecv.at[d], lz_sem.at[d])
        total = total + zrecv[d].astype(jnp.float32)

    new_first = first_decay * first + (1.0 - first_decay) * total
    new_second = second_decay * second + (1.0 - second_decay) * total * total
    ratio = new_first / (jnp.sqrt(new_second) + epsilon)
    rbuf[own] = ratio.astype(jnp.bfloat16)

    gather_z(rbuf, own, send_r, rz_sem)
    for i in range(len(GROUPS)):
        gather_plane(rbuf, own, i, send_r, rz_sem, rxy_sem)

    for d, (i, k) in GROUP_OF.items():
        column[lax.rem(z + d, NZ), :, 0:LANES] = rbuf[BASE[i] + own * len(GROUPS[i]) + k]
    tile = column[:, :, 0:LANES].reshape(RANK, LANES)
    mixed = (
        jnp.dot(gram_1, tile, preferred_element_type=jnp.float32)
        + jnp.dot(gram_2, tile, preferred_element_type=jnp.float32)
        + jnp.dot(gram_3, tile, preferred_element_type=jnp.float32)
    )
    square[...] = jnp.sum(mixed * tile.astype(jnp.float32), axis=0, keepdims=True)
    mine = squares.at[tp * PEERS + own]
    for dx, dy in PLANE:
        device = plane_peer(dx, dy)[2]
        send(square, mine, send_q, q_sem, device)
        send(square, mine, send_q, q_sem, {**device, "tp": 1 - tp})
    send(square, mine, send_q, q_sem, {"tp": 1 - tp})
    squares[tp * PEERS + own] = square[...]

    for i in range(NX):
        lg_send[i, 0:OWNED, :] = total[i * OWNED:(i + 1) * OWNED, :]
    lg_recv[own, 0:OWNED, :] = lg_send[x, 0:OWNED, :]
    for dx, dy in PLANE:
        px, py, device = plane_peer(dx, dy)
        send(lg_send.at[px], lg_recv.at[own], send_g, g_sem, device)

    for i, group in enumerate(GROUPS):
        blocks = arrived(rbuf, i, rxy_sem)
        for k, d in enumerate(group):
            rows = pl.ds(aligned(lax.rem(z + d, NZ), ROWS), ROWS)
            for j in range(PEERS):
                rat_out[rows, j * LANES:(j + 1) * LANES] = blocks[j, k]
    drain(squares.at[pl.ds(0, 2 * PEERS - 1)], q_sem)
    tot_out[...] = jnp.sum(squares[...], axis=0)
    drain(lg_recv.at[pl.ds(0, PEERS - 1)], g_sem)
    lg_out[...] = lg_recv[...]

    for buf, sem in ((fbuf, send_f), (rbuf, send_r)):
        drain(buf.at[pl.ds(0, NZ - 1)], sem)
        drain(buf.at[pl.ds(0, (PEERS - 1) * NZ)], sem)
    drain(lsend.at[pl.ds(0, PEERS - 1)], send_l)
    drain(zsend.at[pl.ds(0, NZ - 1)], send_z)
    drain(mom_send.at[pl.ds(0, NX - 1)], send_m)
    drain(lg_recv.at[pl.ds(0, PEERS - 1)], send_g)
    drain(squares.at[pl.ds(0, 2 * PEERS - 1)], send_q)


def exchange(saved_input, value_cotangent, factor, first_moment, second_moment):
    bf16, f32 = jnp.bfloat16, jnp.float32
    dma = pltpu.SemaphoreType.DMA
    vmem = pl.BlockSpec(memory_space=pltpu.VMEM)
    hbm = pl.BlockSpec(memory_space=pltpu.HBM)
    return pl.pallas_call(
        exchange_kernel,
        out_shape=(
            jax.ShapeDtypeStruct((RANK, COLS), bf16),
            jax.ShapeDtypeStruct((PEERS, 8, LANES), f32),
            jax.ShapeDtypeStruct((1, LANES), f32),
        ),
        in_specs=[hbm] * 5,
        out_specs=(vmem,) * 3,
        scratch_shapes=[
            pltpu.VMEM((D // (NX * NZ), RANK), bf16),
            pltpu.VMEM((OWNED, COLS), f32),
            pltpu.VMEM((OWNED, COLS), f32),
            pltpu.VMEM((TOKENS, D), bf16),
            pltpu.VMEM((TOKENS, COLS), bf16),
            pltpu.VMEM((NZ * PEERS, ROWS, LANES), bf16),
            pltpu.VMEM((TOKENS, RANK), f32),
            pltpu.VMEM((2 * RANK, TOKENS), bf16),
            pltpu.VMEM((PEERS, NZ, ROWS, LANES), bf16),
            pltpu.VMEM((PEERS, NZ, ROWS, LANES), bf16),
            pltpu.VMEM((NZ, ROWS, LANES), bf16),
            pltpu.VMEM((NZ, ROWS, LANES), bf16),
            pltpu.VMEM((NZ * PEERS, ROWS, LANES), bf16),
            pltpu.VMEM((NZ, ROWS, NX * LANES), bf16),
            pltpu.VMEM((NX, 8, LANES), f32),
            pltpu.VMEM((NX, 8, LANES), f32),
            pltpu.VMEM((NX, 8, LANES), f32),
            pltpu.VMEM((PEERS, 8, LANES), f32),
            pltpu.VMEM((1, LANES), f32),
            pltpu.VMEM((2 * PEERS, 1, LANES), f32),
            dma((5,)),
        ] + [dma] * 7 + [
            dma((NZ,)), dma((len(GROUPS),)), dma((len(PARTS),)), dma((NZ,)), dma((NZ,)), dma((len(GROUPS),)),
        ] + [dma] * 3,
        compiler_params=pltpu.CompilerParams(
            collective_id=0, has_side_effects=True, vmem_limit_bytes=32 * 2**20
        ),
    )(*(
        pltpu.with_memory_space_constraint(a, pltpu.HBM)
        for a in (saved_input, value_cotangent, factor, first_moment, second_moment)
    ))


def update_kernel(
    f_ref, rat_ref, lg_ref, tot_ref, w_ref, fm_ref, sm_ref,
    low_ref, first_ref, second_ref, dir_ref, weight_ref, copy_ref,
):
    total = jnp.sum(tot_ref[...], axis=(0, 1), keepdims=True)
    spread = jnp.sqrt(total / (D * E))
    raw = jnp.dot(f_ref[...], rat_ref[...], preferred_element_type=jnp.float32)
    direction = raw / (spread + 1.0)
    new_weight = w_ref[...] - learn_rate * direction
    dir_ref[...] = direction
    weight_ref[...] = new_weight
    copy_ref[...] = new_weight.astype(jnp.bfloat16)
    for j in range(PEERS):
        cols = slice(j * LANES, (j + 1) * LANES)
        low = lg_ref[j, 0:OWNED, :]
        low_ref[:, cols] = low
        first_ref[:, cols] = first_decay * fm_ref[:, cols] + (1.0 - first_decay) * low
        second_ref[:, cols] = second_decay * sm_ref[:, cols] + (1.0 - second_decay) * low * low


def update(factor, ratio, low, total, weight, first_moment, second_moment):
    f32 = jnp.float32
    rows = factor.shape[0]
    vmem = pl.BlockSpec(memory_space=pltpu.VMEM)
    small = jax.ShapeDtypeStruct((OWNED, COLS), f32)
    large = jax.ShapeDtypeStruct((rows, COLS), f32)
    return pl.pallas_call(
        update_kernel,
        out_shape=(small, small, small, large, large, jax.ShapeDtypeStruct((rows, COLS), jnp.bfloat16)),
        in_specs=[vmem] * 7,
        out_specs=(vmem,) * 6,
        compiler_params=pltpu.CompilerParams(vmem_limit_bytes=8 * 2**20),
    )(factor, ratio, low, total, weight, first_moment, second_moment)


def on_device(saved_input, value_cotangent, factor, weight, first_moment, second_moment):
    ratio, low, total = exchange(saved_input, value_cotangent, factor, first_moment, second_moment)
    return update(factor, ratio, low, total, weight, first_moment, second_moment)


def solution(mesh):
    placed = (
        P(("fs", "rep"), None),
        P(("fs", "rep"), "tp"),
        P("fs", None),
        P("fs", "tp"),
        P("fs", "tp"),
        P("fs", "tp"),
    )
    return jax.shard_map(
        on_device,
        mesh=mesh,
        in_specs=placed,
        out_specs=(P("fs", "tp"),) * 6,
        check_vma=False,
    )
```

```python
import functools

import jax
import jax.numpy as jnp
from jax import lax
from jax.experimental import pallas as pl
from jax.experimental.pallas import tpu as pltpu
from jax.sharding import PartitionSpec as P

MESH = pl.DeviceIdType.MESH
D = 2048
E = 4096
NX, NY, NZ = 4, 4, 8
PEERS = NX * NY
ROWS = 16
LANES = 128
OWNED = ROWS // NX
ZBLOCK = D // NZ
TOKENS = 1024
COLS = 2048
RANK = 128

first_decay = 0.9
second_decay = 0.9
learn_rate = 0.05
epsilon = 1e-08

PLANE = sorted(
    [(dx, dy) for dx in range(NX) for dy in range(NY) if (dx, dy) != (0, 0)],
    key=lambda d: -(min(d[0], NX - d[0]) + min(d[1], NY - d[1])),
)
Z_FAR = [4, 3, 5, 2, 6, 1, 7]
GROUPS = [(0,), (1, 7), (2, 6), (3, 5), (4,)]
BASE = [PEERS * sum(len(g) for g in GROUPS[:i]) for i in range(len(GROUPS))]
GROUP_OF = {d: (i, k) for i, g in enumerate(GROUPS) for k, d in enumerate(g)}
PIECES = 2
PIECE = RANK // PIECES
NEAR = [0, 3, 1, 2]


def aligned(value, multiple):
    return pl.multiple_of(value * multiple, multiple)


def exchange_kernel(
    x_hbm, v_hbm, f_hbm, fm_hbm, sm_hbm,
    rat_out, lg_out, tot_out,
    f_ref, fm_ref, sm_ref, xv, vv, fbuf, p_acc, pt, lsend, lrecv, zbuf, rbuf, low,
    mom_own, mom_z, mom, lg_send, lg_recv, square, squares,
    load_sem, send_f, send_l, send_z, send_r, send_m, send_g, send_q,
    fz_sem, fxy_sem, lxy_sem, lz_sem, rxy_sem, mz_sem, mx_sem, g_sem, q_sem,
):
    fs = lax.axis_index("fs")
    y = lax.axis_index("rep")
    tp = lax.axis_index("tp")
    x = lax.rem(fs, NX)
    z = lax.div(fs, NX)
    own = y * NX + x
    own_f = x * NY + y

    def plane_peer(dx, dy):
        px = lax.rem(x + dx, NX)
        py = lax.rem(y + dy, NY)
        return px, py, {"fs": z * NX + px, "rep": py}

    def z_peer(d):
        return {"fs": lax.rem(z + d, NZ) * NX + x}

    def send(src, dst, send_sem, recv_sem, device):
        pltpu.make_async_remote_copy(
            src_ref=src, dst_ref=dst, send_sem=send_sem, recv_sem=recv_sem,
            device_id=device, device_id_type=MESH,
        ).start()

    def drain(ref, sem):
        pltpu.make_async_copy(ref, ref, sem).wait()

    barrier = pltpu.get_barrier_semaphore()
    for d in Z_FAR:
        pl.semaphore_signal(barrier, inc=1, device_id=z_peer(d), device_id_type=MESH)
    for dx, dy in PLANE:
        device = plane_peer(dx, dy)[2]
        pl.semaphore_signal(barrier, inc=1, device_id=device, device_id_type=MESH)
        pl.semaphore_signal(barrier, inc=1, device_id={**device, "tp": 1 - tp}, device_id_type=MESH)
    pl.semaphore_signal(barrier, inc=1, device_id={"tp": 1 - tp}, device_id_type=MESH)

    load_f = pltpu.make_async_copy(f_hbm, f_ref, load_sem.at[2])
    load_fm = pltpu.make_async_copy(fm_hbm, fm_ref, load_sem.at[3])
    load_sm = pltpu.make_async_copy(sm_hbm, sm_ref, load_sem.at[4])
    load_x = pltpu.make_async_copy(x_hbm, xv, load_sem.at[0])
    load_v = pltpu.make_async_copy(v_hbm, vv, load_sem.at[1])
    for load in (load_f, load_fm, load_sm, load_x, load_v):
        load.start()

    load_f.wait()
    fbuf[own_f] = f_ref[pl.ds(aligned(y, ROWS), ROWS), :]
    load_fm.wait()
    load_sm.wait()
    for px in range(NX):
        cols = pl.ds(aligned(y * NX + px, LANES), LANES)
        mom_own[px, 0:OWNED, :] = fm_ref[:, cols]
        mom_own[px, OWNED:2 * OWNED, :] = sm_ref[:, cols]

    pl.semaphore_wait(barrier, NZ - 1 + 2 * (PEERS - 1) + 1)

    def gather_z(buf, slot, send_sem, z_sem):
        for d in Z_FAR:
            i, k = GROUP_OF[NZ - d]
            dst = buf.at[BASE[i] + slot * len(GROUPS[i]) + k]
            send(buf.at[slot], dst, send_sem, z_sem.at[NZ - d], z_peer(d))

    def gather_plane(buf, slot, i, send_sem, z_sem, plane_sem):
        n = len(GROUPS[i])
        block = buf.at[pl.ds(BASE[i] + slot * n, n)]
        for d in GROUPS[i]:
            if d:
                drain(buf.at[0], z_sem.at[d])
        for dx, dy in PLANE:
            send(block, block, send_sem, plane_sem.at[i], plane_peer(dx, dy)[2])

    def arrived(buf, i, plane_sem):
        n = len(GROUPS[i])
        drain(buf.at[pl.ds(0, (PEERS - 1) * n)], plane_sem.at[i])
        return buf[BASE[i]:BASE[i] + PEERS * n].reshape(PEERS, n, ROWS, LANES)

    gather_z(fbuf, own_f, send_f, fz_sem)
    for i in range(len(GROUPS)):
        gather_plane(fbuf, own_f, i, send_f, fz_sem, fxy_sem)
    for d in Z_FAR:
        send(mom_own, mom_z.at[:, z], send_m, mz_sem, z_peer(d))
    mom_z[:, z] = mom_own[...]

    load_x.wait()
    for i, group in enumerate(GROUPS):
        blocks = arrived(fbuf, i, fxy_sem)
        term = p_acc[...] if i else None
        for k, d in enumerate(group):
            columns = xv[:, pl.ds(aligned(lax.rem(z + d, NZ), ZBLOCK), ZBLOCK)]
            block = blocks[:, k].reshape(ZBLOCK, RANK)
            product = jnp.dot(columns, block, preferred_element_type=jnp.float32)
            term = product if term is None else term + product
        p_acc[...] = term
    projected = p_acc[...]
    upper = projected.astype(jnp.bfloat16)
    lower = (projected - upper.astype(jnp.float32)).astype(jnp.bfloat16)
    pt[0:RANK, :] = upper.T
    pt[RANK:, :] = lower.T

    def rows_of(piece):
        return pl.ds(piece * PIECE, PIECE)

    def send_piece(piece, dy):
        for dx in NEAR[::-1]:
            if dx or dy:
                px, py, device = plane_peer(dx, dy)
                src = lsend.at[py * NX + px, rows_of(piece)]
                send(src, lrecv.at[own, rows_of(piece)], send_l, lxy_sem.at[piece], device)

    load_v.wait()
    chunks = [2, 1, 3, 0]
    for step, dy in enumerate(chunks):
        py = lax.rem(y + dy, NY)
        cols = pl.ds(aligned(py, NX * LANES), NX * LANES)
        both = jnp.dot(pt[...], vv[:, cols], preferred_element_type=jnp.float32)
        terms = (both[0:RANK] + both[RANK:]).astype(jnp.bfloat16)
        for px in range(NX):
            lsend[py * NX + px] = terms[:, px * LANES:(px + 1) * LANES]
        send_piece(0, dy)
        if step == 2:
            send_piece(1, chunks[0])
    for dy in chunks[1:]:
        send_piece(1, dy)
    lrecv[own] = lsend[own]

    drain(mom_z.at[:, pl.ds(0, NZ - 1)], mz_sem)
    for dx in range(1, NX):
        px = lax.rem(x + dx, NX)
        send(mom_z.at[px], mom.at[x], send_m, mx_sem, {"fs": z * NX + px})
    mom[x] = mom_z[x]

    whole = fbuf[...].reshape(D, RANK)
    gram = lax.dot_general(whole, whole, (((0,), (0,)), ((), ())), preferred_element_type=jnp.float32)
    gram_1 = gram.astype(jnp.bfloat16)
    rest = gram - gram_1.astype(jnp.float32)
    gram_2 = rest.astype(jnp.bfloat16)
    gram_3 = (rest - gram_2.astype(jnp.float32)).astype(jnp.bfloat16)

    for piece in range(PIECES):
        drain(lrecv.at[pl.ds(0, PEERS - 1), rows_of(piece)], lxy_sem.at[piece])
        summed = jnp.sum(lrecv[:, piece * PIECE:(piece + 1) * PIECE].astype(jnp.float32), axis=0)
        part = zbuf.at[z, rows_of(piece)]
        zbuf[z, rows_of(piece)] = summed.astype(jnp.bfloat16)
        for d in Z_FAR:
            send(part, part, send_z, lz_sem.at[piece], z_peer(d))

    drain(mom.at[pl.ds(0, NX - 1)], mx_sem)
    per = PIECE // ROWS
    for piece in range(PIECES):
        drain(zbuf.at[pl.ds(0, NZ - 1), rows_of(piece)], lz_sem.at[piece])
        total = jnp.sum(zbuf[:, piece * PIECE:(piece + 1) * PIECE].astype(jnp.float32), axis=0)
        low[piece * per:(piece + 1) * per] = total.reshape(per, ROWS, LANES)
        owners = [(i, zs) for zs in range(piece * per, (piece + 1) * per) for i in range(NX)]
        first = jnp.concatenate([mom[i, zs, 0:OWNED] for i, zs in owners], axis=0)
        second = jnp.concatenate([mom[i, zs, OWNED:2 * OWNED] for i, zs in owners], axis=0)
        new_first = first_decay * first + (1.0 - first_decay) * total
        new_second = second_decay * second + (1.0 - second_decay) * total * total
        ratio = new_first / (jnp.sqrt(new_second) + epsilon)
        rbuf[own, rows_of(piece)] = ratio.astype(jnp.bfloat16)
        part = rbuf.at[own, rows_of(piece)]
        for dx, dy in PLANE:
            send(part, part, send_r, rxy_sem.at[piece], plane_peer(dx, dy)[2])

    tile = rbuf[own]
    mixed = (
        jnp.dot(gram_1, tile, preferred_element_type=jnp.float32)
        + jnp.dot(gram_2, tile, preferred_element_type=jnp.float32)
        + jnp.dot(gram_3, tile, preferred_element_type=jnp.float32)
    )
    square[...] = jnp.sum(mixed * tile.astype(jnp.float32), axis=0, keepdims=True)
    mine = squares.at[tp * PEERS + own]
    for dx, dy in PLANE:
        device = plane_peer(dx, dy)[2]
        send(square, mine, send_q, q_sem, device)
        send(square, mine, send_q, q_sem, {**device, "tp": 1 - tp})
    send(square, mine, send_q, q_sem, {"tp": 1 - tp})
    squares[tp * PEERS + own] = square[...]

    own_rows = low[z]
    for i in range(NX):
        lg_send[i, 0:OWNED, :] = own_rows[i * OWNED:(i + 1) * OWNED, :]
    lg_recv[own, 0:OWNED, :] = lg_send[x, 0:OWNED, :]
    for dx, dy in PLANE:
        px, py, device = plane_peer(dx, dy)
        send(lg_send.at[px], lg_recv.at[own], send_g, g_sem, device)

    for piece in range(PIECES):
        drain(rbuf.at[pl.ds(0, PEERS - 1), rows_of(piece)], rxy_sem.at[piece])
        for j in range(PEERS):
            rat_out[rows_of(piece), j * LANES:(j + 1) * LANES] = rbuf[j, rows_of(piece)]
    drain(squares.at[pl.ds(0, 2 * PEERS - 1)], q_sem)
    tot_out[...] = jnp.sum(squares[...], axis=0)
    drain(lg_recv.at[pl.ds(0, PEERS - 1)], g_sem)
    lg_out[...] = lg_recv[...]

    drain(fbuf.at[pl.ds(0, NZ - 1)], send_f)
    drain(fbuf.at[pl.ds(0, (PEERS - 1) * NZ)], send_f)
    drain(lsend.at[pl.ds(0, PEERS - 1)], send_l)
    drain(zbuf.at[pl.ds(0, NZ - 1)], send_z)
    drain(rbuf.at[pl.ds(0, PEERS - 1)], send_r)
    drain(mom_z.at[:, pl.ds(0, NZ - 1)], send_m)
    drain(mom.at[pl.ds(0, NX - 1)], send_m)
    drain(lg_recv.at[pl.ds(0, PEERS - 1)], send_g)
    drain(squares.at[pl.ds(0, 2 * PEERS - 1)], send_q)


def exchange(saved_input, value_cotangent, factor, first_moment, second_moment):
    bf16, f32 = jnp.bfloat16, jnp.float32
    dma = pltpu.SemaphoreType.DMA
    vmem = pl.BlockSpec(memory_space=pltpu.VMEM)
    hbm = pl.BlockSpec(memory_space=pltpu.HBM)
    return pl.pallas_call(
        exchange_kernel,
        out_shape=(
            jax.ShapeDtypeStruct((RANK, COLS), bf16),
            jax.ShapeDtypeStruct((PEERS, 8, LANES), f32),
            jax.ShapeDtypeStruct((1, LANES), f32),
        ),
        in_specs=[hbm] * 5,
        out_specs=(vmem,) * 3,
        scratch_shapes=[
            pltpu.VMEM((D // (NX * NZ), RANK), bf16),
            pltpu.VMEM((OWNED, COLS), f32),
            pltpu.VMEM((OWNED, COLS), f32),
            pltpu.VMEM((TOKENS, D), bf16),
            pltpu.VMEM((TOKENS, COLS), bf16),
            pltpu.VMEM((NZ * PEERS, ROWS, LANES), bf16),
            pltpu.VMEM((TOKENS, RANK), f32),
            pltpu.VMEM((2 * RANK, TOKENS), bf16),
            pltpu.VMEM((PEERS, RANK, LANES), bf16),
            pltpu.VMEM((PEERS, RANK, LANES), bf16),
            pltpu.VMEM((NZ, RANK, LANES), bf16),
            pltpu.VMEM((PEERS, RANK, LANES), bf16),
            pltpu.VMEM((NZ, ROWS, LANES), f32),
            pltpu.VMEM((NX, 8, LANES), f32),
            pltpu.VMEM((NX, NZ, 8, LANES), f32),
            pltpu.VMEM((NX, NZ, 8, LANES), f32),
            pltpu.VMEM((NX, 8, LANES), f32),
            pltpu.VMEM((PEERS, 8, LANES), f32),
            pltpu.VMEM((1, LANES), f32),
            pltpu.VMEM((2 * PEERS, 1, LANES), f32),
            dma((5,)),
        ] + [dma] * 7 + [
            dma((NZ,)), dma((len(GROUPS),)), dma((PIECES,)), dma((PIECES,)), dma((PIECES,)),
        ] + [dma] * 4,
        compiler_params=pltpu.CompilerParams(
            collective_id=0, has_side_effects=True, vmem_limit_bytes=32 * 2**20
        ),
    )(*(
        pltpu.with_memory_space_constraint(a, pltpu.HBM)
        for a in (saved_input, value_cotangent, factor, first_moment, second_moment)
    ))


def update_kernel(
    f_ref, rat_ref, lg_ref, tot_ref, w_ref, fm_ref, sm_ref,
    low_ref, first_ref, second_ref, dir_ref, weight_ref, copy_ref,
):
    total = jnp.sum(tot_ref[...], axis=(0, 1), keepdims=True)
    spread = jnp.sqrt(total / (D * E))
    raw = jnp.dot(f_ref[...], rat_ref[...], preferred_element_type=jnp.float32)
    direction = raw / (spread + 1.0)
    new_weight = w_ref[...] - learn_rate * direction
    dir_ref[...] = direction
    weight_ref[...] = new_weight
    copy_ref[...] = new_weight.astype(jnp.bfloat16)
    for j in range(PEERS):
        cols = slice(j * LANES, (j + 1) * LANES)
        low = lg_ref[j, 0:OWNED, :]
        low_ref[:, cols] = low
        first_ref[:, cols] = first_decay * fm_ref[:, cols] + (1.0 - first_decay) * low
        second_ref[:, cols] = second_decay * sm_ref[:, cols] + (1.0 - second_decay) * low * low


def update(factor, ratio, low, total, weight, first_moment, second_moment):
    f32 = jnp.float32
    rows = factor.shape[0]
    vmem = pl.BlockSpec(memory_space=pltpu.VMEM)
    small = jax.ShapeDtypeStruct((OWNED, COLS), f32)
    large = jax.ShapeDtypeStruct((rows, COLS), f32)
    return pl.pallas_call(
        update_kernel,
        out_shape=(small, small, small, large, large, jax.ShapeDtypeStruct((rows, COLS), jnp.bfloat16)),
        in_specs=[vmem] * 7,
        out_specs=(vmem,) * 6,
        compiler_params=pltpu.CompilerParams(vmem_limit_bytes=8 * 2**20),
    )(factor, ratio, low, total, weight, first_moment, second_moment)


def on_device(saved_input, value_cotangent, factor, weight, first_moment, second_moment):
    ratio, low, total = exchange(saved_input, value_cotangent, factor, first_moment, second_moment)
    return update(factor, ratio, low, total, weight, first_moment, second_moment)


def solution(mesh):
    placed = (
        P(("fs", "rep"), None),
        P(("fs", "rep"), "tp"),
        P("fs", None),
        P("fs", "tp"),
        P("fs", "tp"),
        P("fs", "tp"),
    )
    return jax.shard_map(
        on_device,
        mesh=mesh,
        in_specs=placed,
        out_specs=(P("fs", "tp"),) * 6,
        check_vma=False,
    )
```

```python
import functools

import jax
import jax.numpy as jnp
from jax import lax
from jax.experimental import pallas as pl
from jax.experimental.pallas import tpu as pltpu
from jax.sharding import PartitionSpec as P

MESH = pl.DeviceIdType.MESH
D = 2048
E = 4096
NX, NY, NZ = 4, 4, 8
PEERS = NX * NY
ROWS = 16
LANES = 128
OWNED = ROWS // NX
ZBLOCK = D // NZ
TOKENS = 1024
COLS = 2048
RANK = 128

first_decay = 0.9
second_decay = 0.9
learn_rate = 0.05
epsilon = 1e-08

PLANE = sorted(
    [(dx, dy) for dx in range(NX) for dy in range(NY) if (dx, dy) != (0, 0)],
    key=lambda d: -(min(d[0], NX - d[0]) + min(d[1], NY - d[1])),
)
Z_FAR = [4, 3, 5, 2, 6, 1, 7]
GROUPS = [(0,), (1, 7), (2, 6), (3, 5), (4,)]
BASE = [PEERS * sum(len(g) for g in GROUPS[:i]) for i in range(len(GROUPS))]
GROUP_OF = {d: (i, k) for i, g in enumerate(GROUPS) for k, d in enumerate(g)}
PIECES = 4
PIECE = RANK // PIECES
FAR = [2, 1, 3, 0]


def aligned(value, multiple):
    return pl.multiple_of(value * multiple, multiple)


def exchange_kernel(
    x_hbm, v_hbm, f_hbm, fm_hbm, sm_hbm,
    rat_out, lg_out, tot_out,
    f_ref, fm_ref, sm_ref, xv, vv, fbuf, p_acc, pt, lsend, lrecv, zbuf, rbuf, low,
    mom_own, mom_z, mom, lg_send, lg_recv, square, squares, grams,
    load_sem, send_f, send_l, send_z, send_r, send_m, send_g, send_q,
    fz_sem, fxy_sem, lxy_sem, lz_sem, rxy_sem, mz_sem, mx_sem, g_sem, q_sem,
):
    fs = lax.axis_index("fs")
    y = lax.axis_index("rep")
    tp = lax.axis_index("tp")
    x = lax.rem(fs, NX)
    z = lax.div(fs, NX)
    own = y * NX + x
    own_f = x * NY + y

    def plane_peer(dx, dy):
        px = lax.rem(x + dx, NX)
        py = lax.rem(y + dy, NY)
        return px, py, {"fs": z * NX + px, "rep": py}

    def z_peer(d):
        return {"fs": lax.rem(z + d, NZ) * NX + x}

    def send(src, dst, send_sem, recv_sem, device):
        pltpu.make_async_remote_copy(
            src_ref=src, dst_ref=dst, send_sem=send_sem, recv_sem=recv_sem,
            device_id=device, device_id_type=MESH,
        ).start()

    def drain(ref, sem):
        pltpu.make_async_copy(ref, ref, sem).wait()

    barrier = pltpu.get_barrier_semaphore()
    for d in Z_FAR:
        pl.semaphore_signal(barrier, inc=1, device_id=z_peer(d), device_id_type=MESH)
    for dx, dy in PLANE:
        device = plane_peer(dx, dy)[2]
        pl.semaphore_signal(barrier, inc=1, device_id=device, device_id_type=MESH)
        pl.semaphore_signal(barrier, inc=1, device_id={**device, "tp": 1 - tp}, device_id_type=MESH)
    pl.semaphore_signal(barrier, inc=1, device_id={"tp": 1 - tp}, device_id_type=MESH)

    load_f = pltpu.make_async_copy(f_hbm, f_ref, load_sem.at[2])
    load_fm = pltpu.make_async_copy(fm_hbm, fm_ref, load_sem.at[3])
    load_sm = pltpu.make_async_copy(sm_hbm, sm_ref, load_sem.at[4])
    load_x = pltpu.make_async_copy(x_hbm, xv, load_sem.at[0])
    load_v = pltpu.make_async_copy(v_hbm, vv, load_sem.at[1])
    for load in (load_f, load_fm, load_sm, load_x, load_v):
        load.start()

    load_f.wait()
    fbuf[own_f] = f_ref[pl.ds(aligned(y, ROWS), ROWS), :]
    load_fm.wait()
    load_sm.wait()
    for px in range(NX):
        cols = pl.ds(aligned(y * NX + px, LANES), LANES)
        mom_own[px, 0:OWNED, :] = fm_ref[:, cols]
        mom_own[px, OWNED:2 * OWNED, :] = sm_ref[:, cols]

    pl.semaphore_wait(barrier, NZ - 1 + 2 * (PEERS - 1) + 1)

    def gather_z(buf, slot, send_sem, z_sem):
        for d in Z_FAR:
            i, k = GROUP_OF[NZ - d]
            dst = buf.at[BASE[i] + slot * len(GROUPS[i]) + k]
            send(buf.at[slot], dst, send_sem, z_sem.at[NZ - d], z_peer(d))

    def gather_plane(buf, slot, i, send_sem, z_sem, plane_sem):
        n = len(GROUPS[i])
        block = buf.at[pl.ds(BASE[i] + slot * n, n)]
        for d in GROUPS[i]:
            if d:
                drain(buf.at[0], z_sem.at[d])
        for dx, dy in PLANE:
            send(block, block, send_sem, plane_sem.at[i], plane_peer(dx, dy)[2])

    def arrived(buf, i, plane_sem):
        n = len(GROUPS[i])
        drain(buf.at[pl.ds(0, (PEERS - 1) * n)], plane_sem.at[i])
        return buf[BASE[i]:BASE[i] + PEERS * n].reshape(PEERS, n, ROWS, LANES)

    gather_z(fbuf, own_f, send_f, fz_sem)
    for i in range(len(GROUPS)):
        gather_plane(fbuf, own_f, i, send_f, fz_sem, fxy_sem)
    for d in Z_FAR:
        send(mom_own, mom_z.at[:, z], send_m, mz_sem, z_peer(d))
    mom_z[:, z] = mom_own[...]

    load_x.wait()
    for i, group in enumerate(GROUPS):
        blocks = arrived(fbuf, i, fxy_sem)
        term = p_acc[...] if i else None
        for k, d in enumerate(group):
            columns = xv[:, pl.ds(aligned(lax.rem(z + d, NZ), ZBLOCK), ZBLOCK)]
            block = blocks[:, k].reshape(ZBLOCK, RANK)
            product = jnp.dot(columns, block, preferred_element_type=jnp.float32)
            term = product if term is None else term + product
        p_acc[...] = term
    pt[...] = p_acc[...].astype(jnp.bfloat16).T

    def rows_of(piece):
        return pl.ds(piece * PIECE, PIECE)

    def send_piece(piece, dy, near):
        for dx in near:
            px, py, device = plane_peer(dx, dy)
            src = lsend.at[py * NX + px, rows_of(piece)]
            send(src, lrecv.at[own, rows_of(piece)], send_l, lxy_sem.at[piece], device)

    def terms_of(dy):
        py = lax.rem(y + dy, NY)
        cols = pl.ds(aligned(py, NX * LANES), NX * LANES)
        terms = jnp.dot(pt[...], vv[:, cols], preferred_element_type=jnp.float32)
        for px in range(NX):
            tile = terms[:, px * LANES:(px + 1) * LANES]
            lsend[py * NX + px] = tile.astype(jnp.bfloat16)

    load_v.wait()

    @pl.loop(0, NY - 1)
    def _(step):
        dy = lax.rem(2 + 3 * step + 3 * lax.div(step * (step - 1), 2), NY)
        terms_of(dy)
        send_piece(0, dy, FAR)

    terms_of(0)
    send_piece(0, 0, FAR[:-1])
    for piece in range(1, PIECES):
        for dy in (2, 1, 3):
            send_piece(piece, dy, FAR)
        send_piece(piece, 0, FAR[:-1])
    lrecv[own] = lsend[own]

    drain(mom_z.at[:, pl.ds(0, NZ - 1)], mz_sem)
    for dx in range(1, NX):
        px = lax.rem(x + dx, NX)
        send(mom_z.at[px], mom.at[x], send_m, mx_sem, {"fs": z * NX + px})
    mom[x] = mom_z[x]

    whole = fbuf[...].reshape(D, RANK)
    gram = lax.dot_general(whole, whole, (((0,), (0,)), ((), ())), preferred_element_type=jnp.float32)
    gram_1 = gram.astype(jnp.bfloat16)
    rest = gram - gram_1.astype(jnp.float32)
    gram_2 = rest.astype(jnp.bfloat16)
    gram_3 = (rest - gram_2.astype(jnp.float32)).astype(jnp.bfloat16)
    grams[0:RANK] = gram_1
    grams[RANK:2 * RANK] = gram_2
    grams[2 * RANK:] = gram_3

    for piece in range(PIECES):
        drain(lrecv.at[pl.ds(0, PEERS - 1), rows_of(piece)], lxy_sem.at[piece])
        summed = jnp.sum(lrecv[:, piece * PIECE:(piece + 1) * PIECE].astype(jnp.float32), axis=0)
        part = zbuf.at[z, rows_of(piece)]
        zbuf[z, rows_of(piece)] = summed.astype(jnp.bfloat16)
        for d in Z_FAR:
            send(part, part, send_z, lz_sem.at[piece], z_peer(d))

    drain(mom.at[pl.ds(0, NX - 1)], mx_sem)
    per = PIECE // ROWS
    for piece in range(PIECES):
        drain(zbuf.at[pl.ds(0, NZ - 1), rows_of(piece)], lz_sem.at[piece])
        total = jnp.sum(zbuf[:, piece * PIECE:(piece + 1) * PIECE].astype(jnp.float32), axis=0)
        low[piece * per:(piece + 1) * per] = total.reshape(per, ROWS, LANES)
        owners = [(i, zs) for zs in range(piece * per, (piece + 1) * per) for i in range(NX)]
        first = jnp.concatenate([mom[i, zs, 0:OWNED] for i, zs in owners], axis=0)
        second = jnp.concatenate([mom[i, zs, OWNED:2 * OWNED] for i, zs in owners], axis=0)
        new_first = first_decay * first + (1.0 - first_decay) * total
        new_second = second_decay * second + (1.0 - second_decay) * total * total
        ratio = new_first / (jnp.sqrt(new_second) + epsilon)
        rbuf[own, rows_of(piece)] = ratio.astype(jnp.bfloat16)
        part = rbuf.at[own, rows_of(piece)]
        for dx, dy in PLANE:
            send(part, part, send_r, rxy_sem.at[piece], plane_peer(dx, dy)[2])

    tile = rbuf[own]
    mixed = jnp.dot(grams[...], tile, preferred_element_type=jnp.float32)
    mixed = mixed[0:RANK] + mixed[RANK:2 * RANK] + mixed[2 * RANK:]
    square[...] = jnp.sum(mixed * tile.astype(jnp.float32), axis=0, keepdims=True)
    mine = squares.at[tp * PEERS + own]
    for dx, dy in PLANE:
        device = plane_peer(dx, dy)[2]
        send(square, mine, send_q, q_sem, device)
        send(square, mine, send_q, q_sem, {**device, "tp": 1 - tp})
    send(square, mine, send_q, q_sem, {"tp": 1 - tp})
    squares[tp * PEERS + own] = square[...]

    own_rows = low[z]
    for i in range(NX):
        lg_send[i, 0:OWNED, :] = own_rows[i * OWNED:(i + 1) * OWNED, :]
    lg_recv[own, 0:OWNED, :] = lg_send[x, 0:OWNED, :]
    for dx, dy in PLANE:
        px, py, device = plane_peer(dx, dy)
        send(lg_send.at[px], lg_recv.at[own], send_g, g_sem, device)

    for piece in range(PIECES):
        drain(rbuf.at[pl.ds(0, PEERS - 1), rows_of(piece)], rxy_sem.at[piece])
        for j in range(PEERS):
            rat_out[rows_of(piece), j * LANES:(j + 1) * LANES] = rbuf[j, rows_of(piece)]
    drain(squares.at[pl.ds(0, 2 * PEERS - 1)], q_sem)
    tot_out[...] = jnp.sum(squares[...], axis=0)
    drain(lg_recv.at[pl.ds(0, PEERS - 1)], g_sem)
    lg_out[...] = lg_recv[...]

    drain(fbuf.at[pl.ds(0, NZ - 1)], send_f)
    drain(fbuf.at[pl.ds(0, (PEERS - 1) * NZ)], send_f)
    drain(lsend.at[pl.ds(0, PEERS - 1)], send_l)
    drain(zbuf.at[pl.ds(0, NZ - 1)], send_z)
    drain(rbuf.at[pl.ds(0, PEERS - 1)], send_r)
    drain(mom_z.at[:, pl.ds(0, NZ - 1)], send_m)
    drain(mom.at[pl.ds(0, NX - 1)], send_m)
    drain(lg_recv.at[pl.ds(0, PEERS - 1)], send_g)
    drain(squares.at[pl.ds(0, 2 * PEERS - 1)], send_q)


def exchange(saved_input, value_cotangent, factor, first_moment, second_moment):
    bf16, f32 = jnp.bfloat16, jnp.float32
    dma = pltpu.SemaphoreType.DMA
    vmem = pl.BlockSpec(memory_space=pltpu.VMEM)
    hbm = pl.BlockSpec(memory_space=pltpu.HBM)
    return pl.pallas_call(
        exchange_kernel,
        out_shape=(
            jax.ShapeDtypeStruct((RANK, COLS), bf16),
            jax.ShapeDtypeStruct((PEERS, 8, LANES), f32),
            jax.ShapeDtypeStruct((1, LANES), f32),
        ),
        in_specs=[hbm] * 5,
        out_specs=(vmem,) * 3,
        scratch_shapes=[
            pltpu.VMEM((D // (NX * NZ), RANK), bf16),
            pltpu.VMEM((OWNED, COLS), f32),
            pltpu.VMEM((OWNED, COLS), f32),
            pltpu.VMEM((TOKENS, D), bf16),
            pltpu.VMEM((TOKENS, COLS), bf16),
            pltpu.VMEM((NZ * PEERS, ROWS, LANES), bf16),
            pltpu.VMEM((TOKENS, RANK), f32),
            pltpu.VMEM((RANK, TOKENS), bf16),
            pltpu.VMEM((PEERS, RANK, LANES), bf16),
            pltpu.VMEM((PEERS, RANK, LANES), bf16),
            pltpu.VMEM((NZ, RANK, LANES), bf16),
            pltpu.VMEM((PEERS, RANK, LANES), bf16),
            pltpu.VMEM((NZ, ROWS, LANES), f32),
            pltpu.VMEM((NX, 8, LANES), f32),
            pltpu.VMEM((NX, NZ, 8, LANES), f32),
            pltpu.VMEM((NX, NZ, 8, LANES), f32),
            pltpu.VMEM((NX, 8, LANES), f32),
            pltpu.VMEM((PEERS, 8, LANES), f32),
            pltpu.VMEM((1, LANES), f32),
            pltpu.VMEM((2 * PEERS, 1, LANES), f32),
            pltpu.VMEM((3 * RANK, RANK), bf16),
            dma((5,)),
        ] + [dma] * 7 + [
            dma((NZ,)), dma((len(GROUPS),)), dma((PIECES,)), dma((PIECES,)), dma((PIECES,)),
        ] + [dma] * 4,
        compiler_params=pltpu.CompilerParams(
            collective_id=0, has_side_effects=True, vmem_limit_bytes=32 * 2**20
        ),
    )(*(
        pltpu.with_memory_space_constraint(a, pltpu.HBM)
        for a in (saved_input, value_cotangent, factor, first_moment, second_moment)
    ))


def update_kernel(
    f_ref, rat_ref, lg_ref, tot_ref, w_ref, fm_ref, sm_ref,
    low_ref, first_ref, second_ref, dir_ref, weight_ref, copy_ref,
):
    total = jnp.sum(tot_ref[...], axis=(0, 1), keepdims=True)
    spread = jnp.sqrt(total / (D * E))
    raw = jnp.dot(f_ref[...], rat_ref[...], preferred_element_type=jnp.float32)
    direction = raw / (spread + 1.0)
    new_weight = w_ref[...] - learn_rate * direction
    dir_ref[...] = direction
    weight_ref[...] = new_weight
    copy_ref[...] = new_weight.astype(jnp.bfloat16)
    for j in range(PEERS):
        cols = slice(j * LANES, (j + 1) * LANES)
        low = lg_ref[j, 0:OWNED, :]
        low_ref[:, cols] = low
        first_ref[:, cols] = first_decay * fm_ref[:, cols] + (1.0 - first_decay) * low
        second_ref[:, cols] = second_decay * sm_ref[:, cols] + (1.0 - second_decay) * low * low


def update(factor, ratio, low, total, weight, first_moment, second_moment):
    f32 = jnp.float32
    rows = factor.shape[0]
    vmem = pl.BlockSpec(memory_space=pltpu.VMEM)
    small = jax.ShapeDtypeStruct((OWNED, COLS), f32)
    large = jax.ShapeDtypeStruct((rows, COLS), f32)
    return pl.pallas_call(
        update_kernel,
        out_shape=(small, small, small, large, large, jax.ShapeDtypeStruct((rows, COLS), jnp.bfloat16)),
        in_specs=[vmem] * 7,
        out_specs=(vmem,) * 6,
        compiler_params=pltpu.CompilerParams(vmem_limit_bytes=8 * 2**20),
    )(factor, ratio, low, total, weight, first_moment, second_moment)


def on_device(saved_input, value_cotangent, factor, weight, first_moment, second_moment):
    ratio, low, total = exchange(saved_input, value_cotangent, factor, first_moment, second_moment)
    return update(factor, ratio, low, total, weight, first_moment, second_moment)


def solution(mesh):
    placed = (
        P(("fs", "rep"), None),
        P(("fs", "rep"), "tp"),
        P("fs", None),
        P("fs", "tp"),
        P("fs", "tp"),
        P("fs", "tp"),
    )
    return jax.shard_map(
        on_device,
        mesh=mesh,
        in_specs=placed,
        out_specs=(P("fs", "tp"),) * 6,
        check_vma=False,
    )
```

```python
import functools

import jax
import jax.numpy as jnp
from jax import lax
from jax.experimental import pallas as pl
from jax.experimental.pallas import tpu as pltpu
from jax.sharding import PartitionSpec as P

MESH = pl.DeviceIdType.MESH
D = 2048
E = 4096
NX, NY, NZ = 4, 4, 8
PEERS = NX * NY
ROWS = 16
LANES = 128
OWNED = ROWS // NX
ZBLOCK = D // NZ
TOKENS = 1024
COLS = 2048
RANK = 128

first_decay = 0.9
second_decay = 0.9
learn_rate = 0.05
epsilon = 1e-08

PLANE = sorted(
    [(dx, dy) for dx in range(NX) for dy in range(NY) if (dx, dy) != (0, 0)],
    key=lambda d: -(min(d[0], NX - d[0]) + min(d[1], NY - d[1])),
)
Z_FAR = [4, 3, 5, 2, 6, 1, 7]
GROUPS = [(0,), (1, 7), (2, 6), (3, 5), (4,)]
BASE = [PEERS * sum(len(g) for g in GROUPS[:i]) for i in range(len(GROUPS))]
GROUP_OF = {d: (i, k) for i, g in enumerate(GROUPS) for k, d in enumerate(g)}
SIZES = [64, 32, 32]
PIECES = len(SIZES)
STARTS = [sum(SIZES[:i]) for i in range(PIECES)]
AHEAD = 0
FAR = [2, 1, 3, 0]


def aligned(value, multiple):
    return pl.multiple_of(value * multiple, multiple)


def exchange_kernel(
    x_hbm, v_hbm, f_hbm, fm_hbm, sm_hbm,
    rat_out, lg_out, tot_out,
    f_ref, fm_ref, sm_ref, xv, vv, fbuf, p_acc, pt, lsend, lrecv, zbuf, rbuf, low,
    mom_own, mom_z, mom, lg_send, lg_recv, square, squares, grams,
    load_sem, send_f, send_l, send_z, send_r, send_m, send_g, send_q,
    fz_sem, fxy_sem, lxy_sem, lz_sem, rxy_sem, mz_sem, mx_sem, g_sem, q_sem,
):
    fs = lax.axis_index("fs")
    y = lax.axis_index("rep")
    tp = lax.axis_index("tp")
    x = lax.rem(fs, NX)
    z = lax.div(fs, NX)
    own = y * NX + x
    own_f = x * NY + y

    def plane_peer(dx, dy):
        px = lax.rem(x + dx, NX)
        py = lax.rem(y + dy, NY)
        return px, py, {"fs": z * NX + px, "rep": py}

    def z_peer(d):
        return {"fs": lax.rem(z + d, NZ) * NX + x}

    def send(src, dst, send_sem, recv_sem, device):
        pltpu.make_async_remote_copy(
            src_ref=src, dst_ref=dst, send_sem=send_sem, recv_sem=recv_sem,
            device_id=device, device_id_type=MESH,
        ).start()

    def drain(ref, sem):
        pltpu.make_async_copy(ref, ref, sem).wait()

    barrier = pltpu.get_barrier_semaphore()
    for d in Z_FAR:
        pl.semaphore_signal(barrier, inc=1, device_id=z_peer(d), device_id_type=MESH)
    for dx, dy in PLANE:
        device = plane_peer(dx, dy)[2]
        pl.semaphore_signal(barrier, inc=1, device_id=device, device_id_type=MESH)
        pl.semaphore_signal(barrier, inc=1, device_id={**device, "tp": 1 - tp}, device_id_type=MESH)
    pl.semaphore_signal(barrier, inc=1, device_id={"tp": 1 - tp}, device_id_type=MESH)

    load_f = pltpu.make_async_copy(f_hbm, f_ref, load_sem.at[2])
    load_fm = pltpu.make_async_copy(fm_hbm, fm_ref, load_sem.at[3])
    load_sm = pltpu.make_async_copy(sm_hbm, sm_ref, load_sem.at[4])
    load_x = pltpu.make_async_copy(x_hbm, xv, load_sem.at[0])
    load_v = pltpu.make_async_copy(v_hbm, vv, load_sem.at[1])
    for load in (load_f, load_fm, load_sm, load_x, load_v):
        load.start()

    load_f.wait()
    fbuf[own_f] = f_ref[pl.ds(aligned(y, ROWS), ROWS), :]
    load_fm.wait()
    load_sm.wait()
    for px in range(NX):
        cols = pl.ds(aligned(y * NX + px, LANES), LANES)
        mom_own[px, 0:OWNED, :] = fm_ref[:, cols]
        mom_own[px, OWNED:2 * OWNED, :] = sm_ref[:, cols]

    pl.semaphore_wait(barrier, NZ - 1 + 2 * (PEERS - 1) + 1)

    def gather_z(buf, slot, send_sem, z_sem):
        for d in Z_FAR:
            i, k = GROUP_OF[NZ - d]
            dst = buf.at[BASE[i] + slot * len(GROUPS[i]) + k]
            send(buf.at[slot], dst, send_sem, z_sem.at[NZ - d], z_peer(d))

    def gather_plane(buf, slot, i, send_sem, z_sem, plane_sem):
        n = len(GROUPS[i])
        block = buf.at[pl.ds(BASE[i] + slot * n, n)]
        for d in GROUPS[i]:
            if d:
                drain(buf.at[0], z_sem.at[d])
        for dx, dy in PLANE:
            send(block, block, send_sem, plane_sem.at[i], plane_peer(dx, dy)[2])

    def arrived(buf, i, plane_sem):
        n = len(GROUPS[i])
        drain(buf.at[pl.ds(0, (PEERS - 1) * n)], plane_sem.at[i])
        return buf[BASE[i]:BASE[i] + PEERS * n].reshape(PEERS, n, ROWS, LANES)

    gather_z(fbuf, own_f, send_f, fz_sem)
    for i in range(len(GROUPS)):
        gather_plane(fbuf, own_f, i, send_f, fz_sem, fxy_sem)
    for d in Z_FAR:
        send(mom_own, mom_z.at[:, z], send_m, mz_sem, z_peer(d))
    mom_z[:, z] = mom_own[...]

    load_x.wait()
    for i, group in enumerate(GROUPS):
        blocks = arrived(fbuf, i, fxy_sem)
        term = p_acc[...] if i else None
        for k, d in enumerate(group):
            columns = xv[:, pl.ds(aligned(lax.rem(z + d, NZ), ZBLOCK), ZBLOCK)]
            block = blocks[:, k].reshape(ZBLOCK, RANK)
            product = jnp.dot(columns, block, preferred_element_type=jnp.float32)
            term = product if term is None else term + product
        p_acc[...] = term
    pt[...] = p_acc[...].astype(jnp.bfloat16).T

    def rows_of(piece):
        return pl.ds(STARTS[piece], SIZES[piece])

    def send_piece(piece, dy, near):
        for dx in near:
            px, py, device = plane_peer(dx, dy)
            src = lsend.at[py * NX + px, rows_of(piece)]
            send(src, lrecv.at[own, rows_of(piece)], send_l, lxy_sem.at[piece], device)

    def terms_of(dy):
        py = lax.rem(y + dy, NY)
        cols = pl.ds(aligned(py, NX * LANES), NX * LANES)
        terms = jnp.dot(pt[...], vv[:, cols], preferred_element_type=jnp.float32)
        for px in range(NX):
            tile = terms[:, px * LANES:(px + 1) * LANES]
            lsend[py * NX + px] = tile.astype(jnp.bfloat16)

    load_v.wait()

    @pl.loop(0, NY - 1)
    def _(step):
        dy = lax.rem(2 + 3 * step + 3 * lax.div(step * (step - 1), 2), NY)
        terms_of(dy)
        send_piece(0, dy, FAR)

    terms_of(0)
    send_piece(0, 0, FAR[:-1])
    for piece in range(1, PIECES):
        for dy in (2, 1, 3):
            send_piece(piece, dy, FAR)
        send_piece(piece, 0, FAR[:-1])
    lrecv[own] = lsend[own]

    drain(mom_z.at[:, pl.ds(0, NZ - 1)], mz_sem)
    for dx in range(1, NX):
        px = lax.rem(x + dx, NX)
        send(mom_z.at[px], mom.at[x], send_m, mx_sem, {"fs": z * NX + px})
    mom[x] = mom_z[x]

    whole = fbuf[...].reshape(D, RANK)
    gram = lax.dot_general(whole, whole, (((0,), (0,)), ((), ())), preferred_element_type=jnp.float32)
    gram_1 = gram.astype(jnp.bfloat16)
    rest = gram - gram_1.astype(jnp.float32)
    gram_2 = rest.astype(jnp.bfloat16)
    gram_3 = (rest - gram_2.astype(jnp.float32)).astype(jnp.bfloat16)
    grams[0:RANK] = gram_1
    grams[RANK:2 * RANK] = gram_2
    grams[2 * RANK:] = gram_3

    for piece in range(PIECES):
        drain(lrecv.at[pl.ds(0, PEERS - 1), rows_of(piece)], lxy_sem.at[piece])
        summed = jnp.sum(lrecv[:, rows_of(piece)].astype(jnp.float32), axis=0)
        part = zbuf.at[z, rows_of(piece)]
        zbuf[z, rows_of(piece)] = summed.astype(jnp.bfloat16)
        for d in Z_FAR:
            send(part, part, send_z, lz_sem.at[piece], z_peer(d))

    drain(mom.at[pl.ds(0, NX - 1)], mx_sem)
    for piece in range(PIECES):
        drain(zbuf.at[pl.ds(0, NZ - 1), rows_of(piece)], lz_sem.at[piece])
        total = jnp.sum(zbuf[:, rows_of(piece)].astype(jnp.float32), axis=0)
        begin, end = STARTS[piece] // ROWS, (STARTS[piece] + SIZES[piece]) // ROWS
        low[begin:end] = total.reshape(end - begin, ROWS, LANES)
        owners = [(i, zs) for zs in range(begin, end) for i in range(NX)]
        first = jnp.concatenate([mom[i, zs, 0:OWNED] for i, zs in owners], axis=0)
        second = jnp.concatenate([mom[i, zs, OWNED:2 * OWNED] for i, zs in owners], axis=0)
        new_first = first_decay * first + (1.0 - first_decay) * total
        new_second = second_decay * second + (1.0 - second_decay) * total * total
        ratio = new_first / (jnp.sqrt(new_second) + epsilon)
        narrow = ratio.astype(jnp.bfloat16)
        rbuf[own, rows_of(piece)] = narrow
        part = rbuf.at[own, rows_of(piece)]
        last = piece == PIECES - 1
        for dx, dy in PLANE[:AHEAD] if last else PLANE:
            send(part, part, send_r, rxy_sem.at[piece], plane_peer(dx, dy)[2])
        weights = grams[:, rows_of(piece)]
        product = jnp.dot(weights, narrow, preferred_element_type=jnp.float32)
        product = product[0:RANK] + product[RANK:2 * RANK] + product[2 * RANK:]
        mixed = product if piece == 0 else mixed + product

    tile = rbuf[own]
    square[...] = jnp.sum(mixed * tile.astype(jnp.float32), axis=0, keepdims=True)
    mine = squares.at[tp * PEERS + own]
    for i, (dx, dy) in enumerate(PLANE):
        device = plane_peer(dx, dy)[2]
        send(square, mine, send_q, q_sem, device)
        send(square, mine, send_q, q_sem, {**device, "tp": 1 - tp})
        if i >= AHEAD:
            send(part, part, send_r, rxy_sem.at[PIECES - 1], device)
    send(square, mine, send_q, q_sem, {"tp": 1 - tp})
    squares[tp * PEERS + own] = square[...]

    own_rows = low[z]
    for i in range(NX):
        lg_send[i, 0:OWNED, :] = own_rows[i * OWNED:(i + 1) * OWNED, :]
    lg_recv[own, 0:OWNED, :] = lg_send[x, 0:OWNED, :]
    for dx, dy in PLANE:
        px, py, device = plane_peer(dx, dy)
        send(lg_send.at[px], lg_recv.at[own], send_g, g_sem, device)

    for piece in range(PIECES):
        drain(rbuf.at[pl.ds(0, PEERS - 1), rows_of(piece)], rxy_sem.at[piece])
        for j in range(PEERS):
            rat_out[rows_of(piece), j * LANES:(j + 1) * LANES] = rbuf[j, rows_of(piece)]
    drain(squares.at[pl.ds(0, 2 * PEERS - 1)], q_sem)
    tot_out[...] = jnp.sum(squares[...], axis=0)
    drain(lg_recv.at[pl.ds(0, PEERS - 1)], g_sem)
    lg_out[...] = lg_recv[...]

    drain(fbuf.at[pl.ds(0, NZ - 1)], send_f)
    drain(fbuf.at[pl.ds(0, (PEERS - 1) * NZ)], send_f)
    drain(lsend.at[pl.ds(0, PEERS - 1)], send_l)
    drain(zbuf.at[pl.ds(0, NZ - 1)], send_z)
    drain(rbuf.at[pl.ds(0, PEERS - 1)], send_r)
    drain(mom_z.at[:, pl.ds(0, NZ - 1)], send_m)
    drain(mom.at[pl.ds(0, NX - 1)], send_m)
    drain(lg_recv.at[pl.ds(0, PEERS - 1)], send_g)
    drain(squares.at[pl.ds(0, 2 * PEERS - 1)], send_q)


def exchange(saved_input, value_cotangent, factor, first_moment, second_moment):
    bf16, f32 = jnp.bfloat16, jnp.float32
    dma = pltpu.SemaphoreType.DMA
    vmem = pl.BlockSpec(memory_space=pltpu.VMEM)
    hbm = pl.BlockSpec(memory_space=pltpu.HBM)
    return pl.pallas_call(
        exchange_kernel,
        out_shape=(
            jax.ShapeDtypeStruct((RANK, COLS), bf16),
            jax.ShapeDtypeStruct((PEERS, 8, LANES), f32),
            jax.ShapeDtypeStruct((1, LANES), f32),
        ),
        in_specs=[hbm] * 5,
        out_specs=(vmem,) * 3,
        scratch_shapes=[
            pltpu.VMEM((D // (NX * NZ), RANK), bf16),
            pltpu.VMEM((OWNED, COLS), f32),
            pltpu.VMEM((OWNED, COLS), f32),
            pltpu.VMEM((TOKENS, D), bf16),
            pltpu.VMEM((TOKENS, COLS), bf16),
            pltpu.VMEM((NZ * PEERS, ROWS, LANES), bf16),
            pltpu.VMEM((TOKENS, RANK), f32),
            pltpu.VMEM((RANK, TOKENS), bf16),
            pltpu.VMEM((PEERS, RANK, LANES), bf16),
            pltpu.VMEM((PEERS, RANK, LANES), bf16),
            pltpu.VMEM((NZ, RANK, LANES), bf16),
            pltpu.VMEM((PEERS, RANK, LANES), bf16),
            pltpu.VMEM((NZ, ROWS, LANES), f32),
            pltpu.VMEM((NX, 8, LANES), f32),
            pltpu.VMEM((NX, NZ, 8, LANES), f32),
            pltpu.VMEM((NX, NZ, 8, LANES), f32),
            pltpu.VMEM((NX, 8, LANES), f32),
            pltpu.VMEM((PEERS, 8, LANES), f32),
            pltpu.VMEM((1, LANES), f32),
            pltpu.VMEM((2 * PEERS, 1, LANES), f32),
            pltpu.VMEM((3 * RANK, RANK), bf16),
            dma((5,)),
        ] + [dma] * 7 + [
            dma((NZ,)), dma((len(GROUPS),)), dma((PIECES,)), dma((PIECES,)), dma((PIECES,)),
        ] + [dma] * 4,
        compiler_params=pltpu.CompilerParams(
            collective_id=0, has_side_effects=True, vmem_limit_bytes=32 * 2**20
        ),
    )(*(
        pltpu.with_memory_space_constraint(a, pltpu.HBM)
        for a in (saved_input, value_cotangent, factor, first_moment, second_moment)
    ))


def update_kernel(
    f_ref, rat_ref, lg_ref, tot_ref, w_ref, fm_ref, sm_ref,
    low_hbm, first_hbm, second_hbm, dir_hbm, weight_hbm, copy_hbm,
    low_ref, first_ref, second_ref, dir_ref, weight_ref, copy_ref, sem,
):
    saves = []

    def save(src, dst):
        copy = pltpu.make_async_copy(src, dst, sem.at[len(saves)])
        copy.start()
        saves.append(copy)

    total = jnp.sum(tot_ref[...], axis=(0, 1), keepdims=True)
    scale = 1.0 / (jnp.sqrt(total / (D * E)) + 1.0)
    for begin, end in ((0, 32), (32, 64)):
        rows = slice(begin, end)
        at = pl.ds(begin, end - begin)
        raw = jnp.dot(f_ref[rows], rat_ref[...], preferred_element_type=jnp.float32)
        direction = raw * scale
        dir_ref[rows] = direction
        save(dir_ref.at[at], dir_hbm.at[at])
        new_weight = w_ref[rows] - learn_rate * direction
        weight_ref[rows] = new_weight
        save(weight_ref.at[at], weight_hbm.at[at])
        copy_ref[rows] = new_weight.astype(jnp.bfloat16)
        save(copy_ref.at[at], copy_hbm.at[at])
    for j in range(PEERS):
        cols = slice(j * LANES, (j + 1) * LANES)
        low = lg_ref[j, 0:OWNED, :]
        low_ref[:, cols] = low
        first_ref[:, cols] = first_decay * fm_ref[:, cols] + (1.0 - first_decay) * low
        second_ref[:, cols] = second_decay * sm_ref[:, cols] + (1.0 - second_decay) * low * low
    save(low_ref, low_hbm)
    save(first_ref, first_hbm)
    save(second_ref, second_hbm)
    for copy in saves:
        copy.wait()


def update(factor, ratio, low, total, weight, first_moment, second_moment):
    f32, bf16 = jnp.float32, jnp.bfloat16
    rows = factor.shape[0]
    vmem = pl.BlockSpec(memory_space=pltpu.VMEM)
    hbm = pl.BlockSpec(memory_space=pltpu.HBM)
    shapes = [((OWNED, COLS), f32)] * 3 + [((rows, COLS), f32)] * 2 + [((rows, COLS), bf16)]
    return pl.pallas_call(
        update_kernel,
        out_shape=tuple(jax.ShapeDtypeStruct(*s) for s in shapes),
        in_specs=[vmem] * 7,
        out_specs=(hbm,) * 6,
        scratch_shapes=[pltpu.VMEM(*s) for s in shapes] + [pltpu.SemaphoreType.DMA((9,))],
        compiler_params=pltpu.CompilerParams(vmem_limit_bytes=8 * 2**20),
    )(factor, ratio, low, total, weight, first_moment, second_moment)


def on_device(saved_input, value_cotangent, factor, weight, first_moment, second_moment):
    ratio, low, total = exchange(saved_input, value_cotangent, factor, first_moment, second_moment)
    return update(factor, ratio, low, total, weight, first_moment, second_moment)


def solution(mesh):
    placed = (
        P(("fs", "rep"), None),
        P(("fs", "rep"), "tp"),
        P("fs", None),
        P("fs", "tp"),
        P("fs", "tp"),
        P("fs", "tp"),
    )
    return jax.shard_map(
        on_device,
        mesh=mesh,
        in_specs=placed,
        out_specs=(P("fs", "tp"),) * 6,
        check_vma=False,
    )
```
